32 devices in a mesh: ra: 4 (over z), cb: 4 (over y, x), dp: 2 (over core).
Axes of the slice: x: 2, y: 2, z: 4, core: 2. Of those that a mesh axis runs over, the one named last changes fastest.
Arguments:
- tokens: bfloat16 [2, 512, 4096], P('dp', None, 'ra'), may hold values from -80 to 80
- pre_gain: float32 [4096], P('ra'), may hold values from 0.1 to 1.9
- w_gate: bfloat16 [4096, 11264], P('ra', 'cb'), may hold values from -0.09375 to 0.09375
- w_up: bfloat16 [4096, 11264], P('ra', 'cb'), may hold values from -0.09375 to 0.09375
- conv_gate: float32 [3, 11264], P(None, 'cb'), may hold values from -3.5 to 3.5
- conv_up: float32 [3, 11264], P(None, 'cb'), may hold values from -3.5 to 3.5
- w_down: bfloat16 [11264, 4096], P('cb', 'ra'), may hold values from -2 to 2
- post_gain: float32 [4096], P('ra'), may hold values from 0.1 to 1.9
Outputs:
- mixed: bfloat16 [2, 512, 4096], P('dp', None, 'ra')
The draws below stay inside these ranges and needn't reach their ends.
All inputs are finite; a program needn't handle non-finite values.
Results may differ from the reference program's by a relative error of at most 0.0064.
Values may be sent and summed in bfloat16 or wider, within the bound.
A program may use at most 128 MiB of HBM per device.

```python
import math
import jax
import jax.numpy as jnp
from jax import lax

D = 4096
FF = 11264
TOK_DEV = 512
SEQS = 2


def column_scales(key, width):
    column = jnp.arange(width, dtype=jnp.float32) / (width - 1)
    return 10.0 ** column * jax.random.uniform(key, (width,), jnp.float32, 0.7, 1.4) / 4.0


def draw_tokens(key, part):
    first, second, third = jax.random.split(jax.random.fold_in(key, 11), 3)
    col_scale = column_scales(second, D)
    base = jnp.clip(jax.random.normal(first, (SEQS, TOK_DEV, D), jnp.float32), -6.0, 6.0)
    row_scale = jnp.exp(jax.random.uniform(third, (SEQS, TOK_DEV, 1), jnp.float32, 0.0, math.log(10.0)))
    return (base * row_scale * col_scale / 3.0).astype(jnp.bfloat16)


def draw_w_down(key, part):
    first, second = jax.random.split(jax.random.fold_in(key, 23), 2)
    col_scale = column_scales(second, D)
    base = jnp.clip(jax.random.normal(first, (FF, D), jnp.float32), -6.0, 6.0)
    return (base * col_scale / math.sqrt(FF)).astype(jnp.bfloat16)


def levels(key, extent, cuts, least, top_value):
    level = 1.0
    for axis_at, shards_of in cuts:
        draws = jax.random.uniform(jax.random.fold_in(jax.random.fold_in(key, 6), axis_at), (shards_of,), jnp.float32, least / len(cuts), top_value / len(cuts))
        level = level * jnp.repeat(jnp.exp(draws), extent[axis_at] // shards_of).reshape((-1,) + (1,) * (len(extent) - 1 - axis_at))
    return level


def normal_values(rng, dims, spread, reach, pieces=(), kind=jnp.bfloat16):
    gain = levels(rng, dims, pieces, -0.22, 0.18) if pieces else 1.0
    entries = jax.random.normal(rng, dims, jnp.float32) * spread * gain
    return jnp.minimum(jnp.maximum(entries, -reach), reach).astype(kind)


def setup_inputs(seed: int = 0) -> dict:
    key_list = jax.random.split(jax.random.key(seed), 9)
    return {
        "tokens": draw_tokens(jax.random.fold_in(key_list[8], 71), 0),
        "pre_gain": jnp.clip(1.0 + 0.18 * jax.random.normal(key_list[1], (D,), jnp.float32), 0.1, 1.9),
        "w_gate": normal_values(key_list[2], (D, FF), D ** -0.5, 0.09375, ((0, 4), (1, 4))),
        "w_up": normal_values(key_list[3], (D, FF), D ** -0.5, 0.09375, ((0, 4), (1, 4))),
        "conv_gate": normal_values(key_list[4], (3, FF), 3 ** -0.5, 3.5, ((1, 4),), jnp.float32),
        "conv_up": normal_values(key_list[5], (3, FF), 3 ** -0.5, 3.5, ((1, 4),), jnp.float32),
        "w_down": draw_w_down(jax.random.fold_in(key_list[8], 71), 0),
        "post_gain": jnp.clip(1.0 + 0.18 * jax.random.normal(key_list[7], (D,), jnp.float32), 0.1, 1.9),
    }


epsilon = 1e-06
residual_scale = 0.125

def shifted_sum(field, tap_weights):
    padded = jnp.pad(field, ((0, 0), (1, 1), (0, 0)))
    return padded[:, :-2] * tap_weights[0] + padded[:, 1:-1] * tap_weights[1] + padded[:, 2:] * tap_weights[2]

def reference(tokens, pre_gain, w_gate, w_up, conv_gate, conv_up, w_down, post_gain):
    seq_count, positions, features = tokens.shape
    values = tokens.astype(jnp.float32)
    pre_scale = lax.rsqrt(lax.optimization_barrier(jnp.mean(values * values, axis=-1, keepdims=True)) + epsilon)
    weighted = (values * pre_gain).astype(jnp.bfloat16).reshape(seq_count * positions, features)
    gate_lin = jnp.dot(weighted, w_gate, preferred_element_type=jnp.float32).reshape(seq_count, positions, -1) * pre_scale
    up_lin = jnp.dot(weighted, w_up, preferred_element_type=jnp.float32).reshape(seq_count, positions, -1) * pre_scale
    gate_conv = shifted_sum(gate_lin, conv_gate)
    up_conv = shifted_sum(up_lin, conv_up)
    hidden = (jax.nn.gelu(gate_conv, approximate=True) * up_conv).astype(jnp.bfloat16)
    branch = jnp.dot(hidden.reshape(seq_count * positions, -1), w_down, preferred_element_type=jnp.float32)
    branch = branch.reshape(seq_count, positions, features)
    post_scale = lax.rsqrt(lax.optimization_barrier(jnp.mean(branch * branch, axis=-1, keepdims=True)) + epsilon)
    mixed = residual_scale * values + branch * post_scale * post_gain
    return mixed.astype(jnp.bfloat16)
```

```python
import functools
import jax
import jax.numpy as jnp
from jax import lax
from jax.experimental import pallas as pl
from jax.experimental.pallas import tpu as pltpu
from jax.sharding import PartitionSpec as P

epsilon = 1e-06
residual_scale = 0.125
LANES = 128
PART = 128
BLOCK = 64
LAG = 4
MESH = pl.DeviceIdType.MESH


def gelu(v):
    return 0.5 * v * (1.0 + jnp.tanh(0.7978845608028654 * (v + 0.044715 * v * v * v)))


class Plan:
    def __init__(self, n, m, rows, chunks):
        self.parts = rows // PART
        self.blocks = rows // BLOCK
        self.partials = chunks * self.parts
        self.early = (chunks * 5) // 11
        reach = LAG * (n - 1)
        self.a = max(self.partials, self.early * self.parts + reach)
        self.b = max(self.a + self.blocks, self.partials + reach)
        self.end = self.b + self.blocks
        self.sum_after = 2
        self.mix_at = self.b + reach + self.sum_after + 2
        self.slots = self.mix_at + self.blocks


def kernel(
    n, m, plan,
    tok_hbm, pre_hbm, wg_hbm, wu_hbm, cg_hbm, cu_hbm, wd_hbm, post_hbm, out_ref,
    tok, pre, cg, cu, post,
    w, wd, xw, rbuf, sbuf, full, hid_a, hid_b, acc, sq_out, sq_in, scale, bsend, brecv, ps_out, ps_in,
    lsem, wsem, dsem, psend, precv, hsend, hrecv, sqs, sqr, bss, bsr, pss, psr, oss, osr,
):
    rows, width = tok.shape
    wire = sbuf.dtype
    chunks = w.shape[1]
    half = chunks * LANES
    parts, blocks = plan.parts, plan.blocks
    early = plan.early
    own_rows = BLOCK // m
    dim_full = width * n
    r = lax.axis_index("ra")
    me = lax.axis_index("cb")
    f32, bf16 = jnp.float32, jnp.bfloat16

    def weight_copies(d, c):
        at = pl.ds(pl.multiple_of(d * half + c * LANES, LANES), LANES)
        return (
            pltpu.make_async_copy(wg_hbm.at[:, at], w.at[d, c, :, pl.ds(0, LANES)], wsem.at[0, d, c]),
            pltpu.make_async_copy(wu_hbm.at[:, at], w.at[d, c, :, pl.ds(LANES, LANES)], wsem.at[1, d, c]),
        )

    tok_copies = [
        pltpu.make_async_copy(tok_hbm.at[pl.ds(q * PART, PART)], tok.at[pl.ds(q * PART, PART)], lsem.at[q])
        for q in range(parts)
    ]
    pre_copy = pltpu.make_async_copy(pre_hbm, pre, lsem.at[parts])
    rest = [
        pltpu.make_async_copy(cg_hbm, cg, lsem.at[parts + 1]),
        pltpu.make_async_copy(cu_hbm, cu, lsem.at[parts + 2]),
        pltpu.make_async_copy(post_hbm, post, lsem.at[parts + 3]),
    ]
    pre_copy.start()
    tok_copies[0].start()
    for d in (0, 1):
        for copy in weight_copies(d, 0):
            copy.start()

    barrier = pltpu.get_barrier_semaphore()
    for k in range(1, n):
        pl.semaphore_signal(barrier, inc=1, device_id={"ra": (r + k) % n}, device_id_type=MESH)
    for k in range(1, m):
        pl.semaphore_signal(barrier, inc=1, device_id={"cb": (me + k) % m}, device_id_type=MESH)

    for copy in tok_copies[1:]:
        copy.start()
    for copy in rest:
        copy.start()

    def fetch(c, carry):
        for d in (0, 1):
            for copy in weight_copies(d, c):
                copy.start()
        return carry

    lax.fori_loop(1, chunks, fetch, 0)
    down_copy = pltpu.make_async_copy(wd_hbm, wd, dsem)
    down_copy.start()

    full[pl.ds(0, 8), :] = jnp.zeros((8, 2 * LANES), f32)
    full[pl.ds(rows + 8, 8), :] = jnp.zeros((8, 2 * LANES), f32)

    def square_copy(end, k):
        return pltpu.make_async_remote_copy(
            src_ref=sq_out, dst_ref=sq_in.at[k],
            send_sem=sqs.at[end], recv_sem=sqr.at[k],
            device_id={"ra": end * (n - 1)}, device_id_type=MESH,
        )

    def send_squares():
        values = tok[...].astype(f32)
        square = values * values
        high = square.astype(bf16)
        low = (square - high.astype(f32)).astype(bf16)
        ones = jnp.ones((8, width), bf16)
        nt = (((1,), (1,)), ((), ()))
        sq_out[...] = lax.dot_general(ones, high, nt, preferred_element_type=f32) + lax.dot_general(
            ones, low, nt, preferred_element_type=f32
        )
        for end in (0, 1):
            @pl.when(r != end * (n - 1))
            def _():
                square_copy(end, r).start()

    def total_scale():
        total = sq_out[...]
        for k in range(n):
            @pl.when(r != k)
            def _():
                square_copy(0, k).wait_recv()
            total = total + jnp.where(r != k, sq_in[k], 0.0)
        inv = lax.rsqrt(total / dim_full + epsilon)
        scale[...] = jnp.concatenate([inv] * (LANES // 8), axis=0).T

    def place(d):
        return r * (1 - d) + (n - 1 - r) * d

    def part_rows(b):
        return pl.ds(pl.multiple_of(b * PART, PART), PART)

    def block_rows(b):
        return pl.ds(pl.multiple_of(b * BLOCK, BLOCK), BLOCK)

    def onward(d):
        return {"ra": (r + 1 - 2 * d + n) % n}

    def partial_copy(d, c, b):
        at = part_rows(b)
        return pltpu.make_async_remote_copy(
            src_ref=sbuf.at[d, c, at], dst_ref=rbuf.at[d, c, at],
            send_sem=psend.at[d, c, b], recv_sem=precv.at[d, c, b],
            device_id=onward(d), device_id_type=MESH,
        )

    def hidden_copy(d, g, b):
        hid = (hid_a, hid_b)[g]
        at = block_rows(b)
        return pltpu.make_async_remote_copy(
            src_ref=hid.at[1 - d, at], dst_ref=hid.at[1 - d, at],
            send_sem=hsend.at[d, g, b], recv_sem=hrecv.at[d, g, b],
            device_id=onward(d), device_id_type=MESH,
        )

    def finish_chunk(d, c):
        at = pl.ds(pl.multiple_of(d * half + c * LANES, LANES), LANES)
        taps_g, taps_u = cg[:, at], cu[:, at]
        for j in range(rows // BLOCK):
            window = full[pl.ds(j * BLOCK, BLOCK + 16), :]
            before = pltpu.roll(window, 1, 0)[8:8 + BLOCK]
            here = window[8:8 + BLOCK]
            after = pltpu.roll(window, BLOCK + 15, 0)[8:8 + BLOCK]
            conv = []
            for side, taps in ((0, taps_g), (1, taps_u)):
                lanes = slice(side * LANES, (side + 1) * LANES)
                conv.append(
                    taps[0:1] * before[:, lanes] + taps[1:2] * here[:, lanes] + taps[2:3] * after[:, lanes]
                )
            value = (gelu(conv[0]) * conv[1]).astype(bf16)

            @pl.when(c < early)
            def _():
                hid_a[d, pl.ds(j * BLOCK, BLOCK), pl.ds(pl.multiple_of(jnp.minimum(c, early - 1) * LANES, LANES), LANES)] = value

            @pl.when(c >= early)
            def _():
                hid_b[d, pl.ds(j * BLOCK, BLOCK), pl.ds(pl.multiple_of(jnp.maximum(c - early, 0) * LANES, LANES), LANES)] = value

    def partial_step(d, i):
        p = place(d)
        c = i // parts
        b = i % parts
        at = part_rows(b)

        @pl.when(b == 0)
        def _():
            for copy in weight_copies(d, c):
                copy.wait()

        own = jnp.dot(xw[at, :], w[d, c], preferred_element_type=f32)

        @pl.when(p == 0)
        def _():
            sbuf[d, c, at] = own.astype(wire)
            partial_copy(d, c, b).start()

        @pl.when((p > 0) & (p < n - 1))
        def _():
            partial_copy(d, c, b).wait_recv()
            sbuf[d, c, at] = (own + rbuf[d, c, at].astype(f32)).astype(wire)
            partial_copy(d, c, b).start()

        @pl.when(p == n - 1)
        def _():
            @pl.when(i == 0)
            def _():
                total_scale()

            partial_copy(d, c, b).wait_recv()
            by = scale[at, :]
            total = own + rbuf[d, c, at].astype(f32)
            to = pl.ds(pl.multiple_of(b * PART + 8, 8), PART)
            full[to, :LANES] = total[:, :LANES] * by
            full[to, LANES:] = total[:, LANES:] * by

            @pl.when(b == parts - 1)
            def _():
                finish_chunk(d, c)

    def hidden_step(d, g, b):
        p = place(d)
        hid = (hid_a, hid_b)[g]

        @pl.when(p > 0)
        def _():
            hidden_copy(d, g, b).wait_recv()

        @pl.when(p < n - 1)
        def _():
            hidden_copy(d, g, b).start()

        at = block_rows(b)
        first = (1 - d) * half + g * early * LANES
        deep = hid.shape[2]
        acc[at, :] += jnp.dot(hid[1 - d, at, :], wd[pl.ds(first, deep), :], preferred_element_type=f32)

    def mine(b):
        return pl.ds(pl.multiple_of(b * BLOCK + me * own_rows, own_rows), own_rows)

    def branch_copy(b, k):
        peer = (me + k) % m
        at = pl.ds(pl.multiple_of(b * BLOCK + peer * own_rows, own_rows), own_rows)
        return pltpu.make_async_remote_copy(
            src_ref=bsend.at[at], dst_ref=brecv.at[b, k],
            send_sem=bss.at[b, k], recv_sem=bsr.at[b, k],
            device_id={"cb": peer}, device_id_type=MESH,
        )

    def post_copy(b, k):
        return pltpu.make_async_remote_copy(
            src_ref=ps_out.at[b], dst_ref=ps_in.at[b, k],
            send_sem=pss.at[b, k], recv_sem=psr.at[b, k],
            device_id={"ra": (r + k) % n}, device_id_type=MESH,
        )

    def out_copy(b, k):
        return pltpu.make_async_remote_copy(
            src_ref=out_ref.at[mine(b)], dst_ref=out_ref.at[mine(b)],
            send_sem=oss.at[b, k], recv_sem=osr.at[b, k],
            device_id={"cb": (me + k) % m}, device_id_type=MESH,
        )

    def send_branch(b):
        at = block_rows(b)
        bsend[at, :] = acc[at, :].astype(wire)
        for k in range(1, m):
            branch_copy(b, k).start()

    def sum_branch(b):
        branch = acc[mine(b), :]
        for k in range(1, m):
            branch_copy(b, k).wait_recv()
            branch = branch + brecv[b, k].astype(f32)
        acc[mine(b), :] = branch
        ps_out[b] = jnp.broadcast_to(jnp.sum(branch * branch, axis=1, keepdims=True), (own_rows, LANES))
        for k in range(1, n):
            post_copy(b, k).start()

    def send_mixed(b):
        total = ps_out[b]
        for k in range(1, n):
            post_copy(b, k).wait_recv()
            total = total + ps_in[b, k]
        inv = lax.rsqrt(total[:, 0:1] / dim_full + epsilon)
        at = mine(b)
        mixed = residual_scale * tok[at, :].astype(f32) + acc[at, :] * inv * post[...]
        out_ref[at, :] = mixed.astype(bf16)
        for k in range(1, m):
            out_copy(b, k).start()

    pre_copy.wait()

    def slot(s, carry):
        @pl.when(s < parts)
        def _():
            q = jnp.minimum(s, parts - 1)
            at = part_rows(q)
            pltpu.make_async_copy(tok_hbm.at[at], tok.at[at], lsem.at[q]).wait()
            xw[at, :] = (tok[at, :].astype(f32) * pre[...]).astype(bf16)

        @pl.when(s == 0)
        def _():
            pl.semaphore_wait(barrier, n - 1 + m - 1)

        @pl.when(s == parts)
        def _():
            for copy in rest:
                copy.wait()
            send_squares()
            acc[...] = jnp.zeros_like(acc)

        @pl.when(s == plan.a)
        def _():
            down_copy.wait()

        for d in (0, 1):
            i = s - LAG * place(d)

            @pl.when((i >= 0) & (i < plan.partials))
            def _():
                partial_step(d, i)

        for d in (0, 1):
            i = s - LAG * place(d)
            for g, first in ((0, plan.a), (1, plan.b)):
                @pl.when((i >= first) & (i < first + blocks))
                def _():
                    hidden_step(d, g, i - first)

        send_at = s - plan.b - LAG * jnp.maximum(r, n - 1 - r)

        @pl.when((send_at >= 0) & (send_at < blocks))
        def _():
            send_branch(send_at)

        sum_at = send_at - plan.sum_after

        @pl.when((sum_at >= 0) & (sum_at < blocks))
        def _():
            sum_branch(sum_at)

        mix_at = s - plan.mix_at

        @pl.when(mix_at >= 0)
        def _():
            send_mixed(mix_at)

        return carry

    lax.fori_loop(0, plan.slots, slot, 0)

    for end in (0, 1):
        @pl.when(r != end * (n - 1))
        def _():
            square_copy(end, r).wait_send()

    for d in (0, 1):
        @pl.when(place(d) < n - 1)
        def _():
            def drain_partials(i, carry):
                partial_copy(d, i // parts, i % parts).wait_send()
                return carry

            def drain_hidden(b, carry):
                for g in (0, 1):
                    hidden_copy(d, g, b).wait_send()
                return carry

            lax.fori_loop(0, plan.partials, drain_partials, 0)
            lax.fori_loop(0, blocks, drain_hidden, 0)

    def drain(b, carry):
        for k in range(1, m):
            branch_copy(b, k).wait_send()
            out_copy(b, k).wait()
        for k in range(1, n):
            post_copy(b, k).wait_send()
        return carry

    lax.fori_loop(0, blocks, drain, 0)


def local(n, m, tokens, pre_gain, w_gate, w_up, conv_gate, conv_up, w_down, post_gain):
    rows, width = tokens.shape[1:]
    chunks = w_gate.shape[1] // (2 * LANES)
    half = chunks * LANES
    plan = Plan(n, m, rows, chunks)
    parts, blocks = plan.parts, plan.blocks
    own_rows = BLOCK // m
    wire = jnp.bfloat16 if n <= 4 else jnp.float32
    f32, bf16 = jnp.float32, jnp.bfloat16
    hbm = pl.BlockSpec(memory_space=pl.ANY)
    dma = pltpu.SemaphoreType.DMA
    out = pl.pallas_call(
        functools.partial(kernel, n, m, plan),
        out_shape=jax.ShapeDtypeStruct((rows, width), bf16),
        in_specs=[hbm] * 8,
        out_specs=pl.BlockSpec(memory_space=pltpu.VMEM),
        scratch_shapes=[
            pltpu.VMEM((rows, width), bf16),
            pltpu.VMEM((1, width), f32),
            pltpu.VMEM(conv_gate.shape, f32),
            pltpu.VMEM(conv_up.shape, f32),
            pltpu.VMEM((1, width), f32),
            pltpu.VMEM((2, chunks, width, 2 * LANES), bf16),
            pltpu.VMEM(w_down.shape, bf16),
            pltpu.VMEM((rows, width), bf16),
            pltpu.VMEM((2, chunks, rows, 2 * LANES), wire),
            pltpu.VMEM((2, chunks, rows, 2 * LANES), wire),
            pltpu.VMEM((rows + 16, 2 * LANES), f32),
            pltpu.VMEM((2, rows, plan.early * LANES), bf16),
            pltpu.VMEM((2, rows, half - plan.early * LANES), bf16),
            pltpu.VMEM((rows, width), f32),
            pltpu.VMEM((8, rows), f32),
            pltpu.VMEM((n, 8, rows), f32),
            pltpu.VMEM((rows, LANES), f32),
            pltpu.VMEM((rows, width), wire),
            pltpu.VMEM((blocks, m, own_rows, width), wire),
            pltpu.VMEM((blocks, own_rows, LANES), f32),
            pltpu.VMEM((blocks, n, own_rows, LANES), f32),
            dma((parts + 4,)), dma((2, 2, chunks)), dma,
            dma((2, chunks, parts)), dma((2, chunks, parts)), dma((2, 2, blocks)), dma((2, 2, blocks)),
            dma((2,)), dma((n,)), dma((blocks, m)), dma((blocks, m)), dma((blocks, n)), dma((blocks, n)),
            dma((blocks, m)), dma((blocks, m)),
        ],
        compiler_params=pltpu.CompilerParams(
            collective_id=0, has_side_effects=True, vmem_limit_bytes=60 * 1024 * 1024
        ),
    )(tokens[0], pre_gain[None], w_gate, w_up, conv_gate, conv_up, w_down, post_gain[None])
    return out[None]


def solution(mesh):
    in_specs = (
        P("dp", None, "ra"),
        P("ra"),
        P("ra", "cb"),
        P("ra", "cb"),
        P(None, "cb"),
        P(None, "cb"),
        P("cb", "ra"),
        P("ra"),
    )
    out_specs = P("dp", None, "ra")
    return jax.shard_map(
        functools.partial(local, mesh.shape["ra"], mesh.shape["cb"]),
        mesh=mesh, in_specs=in_specs, out_specs=out_specs, check_vma=False,
    )
```

```python
import functools
import jax
import jax.numpy as jnp
from jax import lax
from jax.experimental import pallas as pl
from jax.experimental.pallas import tpu as pltpu
from jax.sharding import PartitionSpec as P

epsilon = 1e-06
residual_scale = 0.125
LANES = 128
PART = 128
BLOCK = 64
LAG = 3
LAST_LAG = 5
FIRST = 32
MESH = pl.DeviceIdType.MESH


def gelu(v):
    return 0.5 * v * (1.0 + jnp.tanh(0.7978845608028654 * (v + 0.044715 * v * v * v)))


class Plan:
    def __init__(self, n, rows, chunks):
        self.parts = rows // PART
        self.blocks = rows // BLOCK
        self.partials = chunks * self.parts
        cuts = (0, (chunks * 3) // 11, (chunks * 7) // 11, chunks)
        self.groups = []
        at = self.partials
        for g in range(3):
            size, lag = (BLOCK, LAG) if g < 2 else (BLOCK // 2, LAST_LAG)
            at = max(at, cuts[g + 1] * self.parts - 1 + LAG * (n - 1))
            self.groups.append((cuts[g], cuts[g + 1], size, rows // size, lag, at))
            at += rows // size
        self.done = self.groups[2][5] + 1
        self.sum_after = 8
        self.slots = self.done + LAST_LAG * (n - 1) + self.sum_after + 2 * self.blocks


def kernel(
    n, m, plan,
    tok_hbm, pre_hbm, wg_hbm, wu_hbm, cg_hbm, cu_hbm, wd_hbm, branch_ref, stat_ref,
    tok, pre, cg, cu,
    w, wd, xw, rbuf, sbuf, full, hid_a, hid_b, hid_c, acc, sq_own, sq_out, sq_in, scale, bsend, brecv, bout, stat,
    lsem, wsem, dsem, psend, pfirst, precv, hsend, hrecv, sqs, sqr, bss, bsr, oss, osr, osl, sts, str_, stl,
):
    rows, width = tok.shape
    wire = sbuf.dtype
    chunks = w.shape[1]
    half = chunks * LANES
    parts, blocks = plan.parts, plan.blocks
    hids = (hid_a, hid_b, hid_c)
    own_rows = BLOCK // m
    dim_full = width * n
    r = lax.axis_index("ra")
    me = lax.axis_index("cb")
    f32, bf16 = jnp.float32, jnp.bfloat16
    upper = (2 * r) // n

    def place(d):
        return r * (1 - d) + (n - 1 - r) * d

    def onward(d):
        return {"ra": (r + 1 - 2 * d + n) % n}

    def somewhere(i, k):
        return {"ra": (r + i) % n, "cb": (me + k) % m}

    def weight_copies(d, c):
        at = pl.ds(pl.multiple_of(d * half + c * LANES, LANES), LANES)
        return (
            pltpu.make_async_copy(wg_hbm.at[:, at], w.at[d, c, :, pl.ds(0, LANES)], wsem.at[0, d, c]),
            pltpu.make_async_copy(wu_hbm.at[:, at], w.at[d, c, :, pl.ds(LANES, LANES)], wsem.at[1, d, c]),
        )

    tok_copies = [
        pltpu.make_async_copy(tok_hbm.at[pl.ds(q * PART, PART)], tok.at[pl.ds(q * PART, PART)], lsem.at[q])
        for q in range(parts)
    ]
    pre_copy = pltpu.make_async_copy(pre_hbm, pre, lsem.at[parts])
    rest = [
        pltpu.make_async_copy(cg_hbm, cg, lsem.at[parts + 1]),
        pltpu.make_async_copy(cu_hbm, cu, lsem.at[parts + 2]),
    ]
    pre_copy.start()
    tok_copies[0].start()
    for d in (0, 1):
        for copy in weight_copies(d, 0):
            copy.start()
    for copy in tok_copies[1:]:
        copy.start()

    barrier = pltpu.get_barrier_semaphore()
    others = [(i, k) for k in range(m) for i in range(n) if i or k]

    for d in (0, 1):
        @pl.when(place(d) < n - 1)
        def _():
            pl.semaphore_signal(barrier, inc=1, device_id=onward(d), device_id_type=MESH)

    for k in range(1, m):
        pl.semaphore_signal(barrier, inc=1, device_id=somewhere(0, k), device_id_type=MESH)

    for copy in rest:
        copy.start()

    down_copy = pltpu.make_async_copy(wd_hbm, wd, dsem)

    def fetch(c):
        for d in (0, 1):
            for copy in weight_copies(d, c):
                copy.start()

    fetch(1)
    full[pl.ds(0, 8), :] = jnp.zeros((8, 2 * LANES), f32)
    full[pl.ds(rows + 8, 8), :] = jnp.zeros((8, 2 * LANES), f32)
    scale[pl.ds(0, 8), :] = jnp.zeros((8, LANES), f32)
    scale[pl.ds(rows + 8, 8), :] = jnp.zeros((8, LANES), f32)

    def square_copy(d):
        return pltpu.make_async_remote_copy(
            src_ref=sq_out.at[d], dst_ref=sq_in.at[d],
            send_sem=sqs.at[d], recv_sem=sqr.at[d],
            device_id=onward(d), device_id_type=MESH,
        )

    def own_squares():
        values = tok[...].astype(f32)
        square = values * values
        high = square.astype(bf16)
        low = (square - high.astype(f32)).astype(bf16)
        ones = jnp.ones((8, width), bf16)
        nt = (((1,), (1,)), ((), ()))
        sq_own[...] = lax.dot_general(ones, high, nt, preferred_element_type=f32) + lax.dot_general(
            ones, low, nt, preferred_element_type=f32
        )

    def square_step(d):
        p = place(d)

        @pl.when(p == 0)
        def _():
            sq_out[d] = sq_own[...]

        @pl.when(p > 0)
        def _():
            square_copy(d).wait_recv()
            sq_out[d] = sq_own[...] + sq_in[d]

        @pl.when(p < n - 1)
        def _():
            square_copy(d).start()

        @pl.when(p == n - 1)
        def _():
            inv = lax.rsqrt(sq_out[d] / dim_full + epsilon)
            scale[pl.ds(8, rows), :] = jnp.concatenate([inv] * (LANES // 8), axis=0).T

    def part_rows(b):
        return pl.ds(pl.multiple_of(b * PART, PART), PART)

    def block_rows(b):
        return pl.ds(pl.multiple_of(b * BLOCK, BLOCK), BLOCK)

    def partial_copy(d, c, b):
        at = part_rows(b)
        return pltpu.make_async_remote_copy(
            src_ref=sbuf.at[d, c, at], dst_ref=rbuf.at[d, c, at],
            send_sem=psend.at[d], recv_sem=precv.at[d, c, b],
            device_id=onward(d), device_id_type=MESH,
        )

    def first_copy(d, b, j):
        at = pl.ds(pl.multiple_of(b * PART + j * FIRST, FIRST), FIRST)
        return pltpu.make_async_remote_copy(
            src_ref=sbuf.at[d, 0, at], dst_ref=rbuf.at[d, 0, at],
            send_sem=psend.at[d], recv_sem=pfirst.at[d, b, j],
            device_id=onward(d), device_id_type=MESH,
        )

    def hidden_copy(d, g, b):
        hid = hids[g]
        size = plan.groups[g][2]
        at = pl.ds(pl.multiple_of(b * size, size), size)
        return pltpu.make_async_remote_copy(
            src_ref=hid.at[1 - d, at], dst_ref=hid.at[1 - d, at],
            send_sem=hsend.at[d, g], recv_sem=hrecv.at[d, g, b],
            device_id=onward(d), device_id_type=MESH,
        )

    def finish_chunk(d, c):
        at = pl.ds(pl.multiple_of(d * half + c * LANES, LANES), LANES)
        taps_g, taps_u = cg[:, at], cu[:, at]
        for j in range(rows // BLOCK):
            by = scale[pl.ds(j * BLOCK, BLOCK + 16), :]
            window = full[pl.ds(j * BLOCK, BLOCK + 16), :] * jnp.concatenate([by, by], axis=1)
            before = pltpu.roll(window, 1, 0)[8:8 + BLOCK]
            here = window[8:8 + BLOCK]
            after = pltpu.roll(window, BLOCK + 15, 0)[8:8 + BLOCK]
            conv = []
            for side, taps in ((0, taps_g), (1, taps_u)):
                lanes = slice(side * LANES, (side + 1) * LANES)
                conv.append(
                    taps[0:1] * before[:, lanes] + taps[1:2] * here[:, lanes] + taps[2:3] * after[:, lanes]
                )
            value = (gelu(conv[0]) * conv[1]).astype(bf16)

            for hid, (low, high, *_) in zip(hids, plan.groups):
                @pl.when((c >= low) & (c < high))
                def _():
                    spot = jnp.clip(c - low, 0, high - low - 1)
                    hid[d, pl.ds(j * BLOCK, BLOCK), pl.ds(pl.multiple_of(spot * LANES, LANES), LANES)] = value

    def partial_step(d, i):
        p = place(d)
        c = i // parts
        b = i % parts
        at = part_rows(b)

        @pl.when(b == 0)
        def _():
            for copy in weight_copies(d, c):
                copy.wait()

        own = jnp.dot(xw[at, :], w[d, c], preferred_element_type=f32)

        @pl.when((p < n - 1) & (c == 0))
        def _():
            for j in range(PART // FIRST):
                some = pl.ds(pl.multiple_of(b * PART + j * FIRST, FIRST), FIRST)
                piece = own[j * FIRST:(j + 1) * FIRST]

                @pl.when(p == 0)
                def _():
                    sbuf[d, 0, some] = piece.astype(wire)

                @pl.when(p > 0)
                def _():
                    first_copy(d, b, j).wait_recv()
                    sbuf[d, 0, some] = (piece + rbuf[d, 0, some].astype(f32)).astype(wire)

                first_copy(d, b, j).start()

        @pl.when((p == 0) & (c > 0))
        def _():
            sbuf[d, c, at] = own.astype(wire)
            partial_copy(d, c, b).start()

        @pl.when((p > 0) & (p < n - 1) & (c > 0))
        def _():
            partial_copy(d, c, b).wait_recv()
            sbuf[d, c, at] = (own + rbuf[d, c, at].astype(f32)).astype(wire)
            partial_copy(d, c, b).start()

        @pl.when(p == n - 1)
        def _():
            @pl.when(c == 0)
            def _():
                for j in range(PART // FIRST):
                    first_copy(d, b, j).wait_recv()

            @pl.when(c > 0)
            def _():
                partial_copy(d, c, b).wait_recv()

            full[pl.ds(pl.multiple_of(b * PART + 8, 8), PART), :] = own + rbuf[d, c, at].astype(f32)

            @pl.when(b == parts - 1)
            def _():
                finish_chunk(d, c)

    def hidden_step(d, g, k):
        p = place(d)
        hid = hids[g]
        low, high, size = plan.groups[g][:3]
        first_row = pl.multiple_of((1 - d) * half + low * LANES, LANES)

        @pl.when(p > 0)
        def _():
            hidden_copy(d, g, k).wait_recv()

        @pl.when((p > 0) & (p < n - 1))
        def _():
            hidden_copy(d, g, k).start()

        every = BLOCK // size

        @pl.when(k % every == every - 1)
        def _():
            at = block_rows(k // every)
            acc[at, :] += jnp.dot(
                hid[1 - d, at, :], wd[pl.ds(first_row, (high - low) * LANES), :],
                preferred_element_type=f32,
            )

    def mine(b):
        return pl.ds(pl.multiple_of(b * BLOCK + me * own_rows, own_rows), own_rows)

    def branch_copy(b, k):
        peer = (me + k) % m
        at = pl.ds(pl.multiple_of(b * BLOCK + peer * own_rows, own_rows), own_rows)
        return pltpu.make_async_remote_copy(
            src_ref=bsend.at[at], dst_ref=brecv.at[k, b],
            send_sem=bss.at[k], recv_sem=bsr.at[b, k],
            device_id={"cb": peer}, device_id_type=MESH,
        )

    def out_copy(b, k):
        return pltpu.make_async_remote_copy(
            src_ref=bout.at[b], dst_ref=branch_ref.at[mine(b)],
            send_sem=oss.at[k], recv_sem=osr.at[k],
            device_id={"cb": (me + k) % m}, device_id_type=MESH,
        )

    def stat_copy(i, k):
        return pltpu.make_async_remote_copy(
            src_ref=stat, dst_ref=stat_ref.at[r * m + me],
            send_sem=sts.at[i, k], recv_sem=str_.at[i, k],
            device_id=somewhere(i, k), device_id_type=MESH,
        )

    keep_stat = pltpu.make_async_copy(stat, stat_ref.at[r * m + me], stl)

    def send_branch(b):
        at = block_rows(b)
        bsend[at, :] = acc[at, :].astype(wire)
        for k in range(1, m):
            branch_copy(b, k).start()

    def sum_branch(b):
        branch = acc[mine(b), :]
        for k in range(1, m):
            branch_copy(b, k).wait_recv()
            branch = branch + brecv[k, b].astype(f32)
        bout[b] = branch.astype(bf16)
        for k in range(1, m):
            out_copy(b, k).start()
        pltpu.make_async_copy(bout.at[b], branch_ref.at[mine(b)], osl).start()
        sums = jnp.sum(branch * branch, axis=1, keepdims=True)
        lanes = stat.shape[1]
        lane = lax.broadcasted_iota(jnp.int32, (own_rows, lanes), 1)
        row = lax.broadcasted_iota(jnp.int32, (own_rows, lanes), 0)
        spread = jnp.sum(jnp.where(lane == b * own_rows + row, sums, 0.0), axis=0, keepdims=True)
        stat[...] = stat[...] + spread

        @pl.when(b == blocks - 1)
        def _():
            for i, k in others:
                stat_copy(i, k).start()
            keep_stat.start()

    pre_copy.wait()

    def slot(s, carry):
        @pl.when(s < parts)
        def _():
            q = jnp.minimum(s, parts - 1)
            at = part_rows(q)
            pltpu.make_async_copy(tok_hbm.at[at], tok.at[at], lsem.at[q]).wait()
            xw[at, :] = (tok[at, :].astype(f32) * pre[...]).astype(bf16)

        @pl.when(s == 0)
        def _():
            pl.semaphore_wait(barrier, jnp.where((r == 0) | (r == n - 1), 1, 2) + m - 1)

        @pl.when(s == parts - 1)
        def _():
            for copy in rest:
                copy.wait()
            own_squares()

        for order in (0, 1):
            d = (order + 1 - upper) % 2
            i = s - LAG * place(d)

            @pl.when(i == parts - 1)
            def _():
                square_step(d)

            @pl.when((i >= 0) & (i < plan.partials))
            def _():
                partial_step(d, i)

        @pl.when((s >= 1) & (s < chunks - 1))
        def _():
            fetch(s + 1)

        @pl.when(s == chunks)
        def _():
            down_copy.start()
            acc[...] = jnp.zeros_like(acc)
            stat[...] = jnp.zeros_like(stat)

        @pl.when(s == plan.partials)
        def _():
            down_copy.wait()

        for g, (_, _, _, count, lag, first) in enumerate(plan.groups):
            for order in (0, 1):
                d = (order + 1 - upper) % 2
                k = s - lag * place(d) - first

                @pl.when((k == 0) & (place(d) == 0))
                def _():
                    def send(j, carry):
                        hidden_copy(d, g, j).start()
                        return carry

                    lax.fori_loop(0, count, send, 0)

                @pl.when((k >= 0) & (k < count))
                def _():
                    hidden_step(d, g, k)

        @pl.when(s == plan.done)
        def _():
            for d in (0, 1):
                @pl.when(place(d) < n - 1)
                def _():
                    pltpu.make_async_remote_copy(
                        src_ref=sbuf.at[d], dst_ref=rbuf.at[d], send_sem=psend.at[d], recv_sem=precv.at[d, 0, 0],
                        device_id=onward(d), device_id_type=MESH,
                    ).wait_send()

        since = s - plan.done - LAST_LAG * jnp.maximum(r, n - 1 - r)
        send_at = since // 2

        @pl.when((since >= 0) & (since % 2 == 0) & (send_at < blocks))
        def _():
            send_branch(send_at)

        since = since - plan.sum_after
        sum_at = since // 2

        @pl.when((since >= 0) & (since % 2 == 0) & (sum_at < blocks))
        def _():
            sum_branch(sum_at)

        return carry

    lax.fori_loop(0, plan.slots, slot, 0)

    for d in (0, 1):
        @pl.when(place(d) < n - 1)
        def _():
            square_copy(d).wait_send()

    for d in (0, 1):
        @pl.when(place(d) < n - 1)
        def _():
            for g in range(3):
                pltpu.make_async_remote_copy(
                    src_ref=hids[g].at[1 - d], dst_ref=hids[g].at[1 - d], send_sem=hsend.at[d, g], recv_sem=hrecv.at[d, g, 0],
                    device_id=onward(d), device_id_type=MESH,
                ).wait_send()

    for k in range(1, m):
        peer = {"cb": (me + k) % m}
        pltpu.make_async_remote_copy(
            src_ref=brecv.at[k], dst_ref=brecv.at[k], send_sem=bss.at[k], recv_sem=bsr.at[0, k],
            device_id=peer, device_id_type=MESH,
        ).wait_send()
        share = branch_ref.at[pl.ds(0, rows // m)]
        pltpu.make_async_remote_copy(
            src_ref=bout, dst_ref=bout, send_sem=oss.at[k], recv_sem=osr.at[k],
            device_id=peer, device_id_type=MESH,
        ).wait_send()
        pltpu.make_async_remote_copy(
            src_ref=share, dst_ref=share, send_sem=oss.at[k], recv_sem=osr.at[k],
            device_id=peer, device_id_type=MESH,
        ).wait_recv()
    share = branch_ref.at[pl.ds(0, rows // m)]
    pltpu.make_async_copy(share, share, osl).wait()
    for i, k in others:
        stat_copy(i, k).wait()
    keep_stat.wait()


def finish_kernel(
    n, m, tok_hbm, branch_hbm, stat_hbm, post_hbm, out_hbm,
    tok, branch, stat, post, scale, out, isem, osem,
):
    rows, width = tok.shape
    parts = rows // PART
    blocks = rows // BLOCK
    own_rows = BLOCK // m
    f32 = jnp.float32
    stat_copy = pltpu.make_async_copy(stat_hbm, stat, isem.at[2 * parts])
    post_copy = pltpu.make_async_copy(post_hbm, post, isem.at[2 * parts + 1])
    stat_copy.start()
    post_copy.start()
    copies = []
    for q in range(parts):
        at = pl.ds(q * PART, PART)
        pair = (
            pltpu.make_async_copy(branch_hbm.at[at], branch.at[at], isem.at[q]),
            pltpu.make_async_copy(tok_hbm.at[at], tok.at[at], isem.at[parts + q]),
        )
        for copy in pair:
            copy.start()
        copies.append(pair)
    stat_copy.wait()
    for k in range(m):
        total = stat[k]
        for i in range(1, n):
            total = total + stat[i * m + k]
        inv = lax.rsqrt(total / (width * n) + epsilon)
        column = jnp.broadcast_to(inv, (LANES, rows // m)).T
        for b in range(blocks):
            scale[pl.ds(b * BLOCK + k * own_rows, own_rows), :] = column[b * own_rows:(b + 1) * own_rows]
    post_copy.wait()
    writes = []
    for q in range(parts):
        for copy in copies[q]:
            copy.wait()
        at = pl.ds(q * PART, PART)
        by = scale[at, :]
        for t in range(width // LANES):
            lanes = pl.ds(t * LANES, LANES)
            mixed = residual_scale * tok[at, lanes].astype(f32) + branch[at, lanes].astype(f32) * by * post[:, lanes]
            out[at, lanes] = mixed.astype(out.dtype)
        write = pltpu.make_async_copy(out.at[at], out_hbm.at[at], osem.at[q])
        write.start()
        writes.append(write)
    for write in writes:
        write.wait()


def local(n, m, tokens, pre_gain, w_gate, w_up, conv_gate, conv_up, w_down, post_gain):
    rows, width = tokens.shape[1:]
    chunks = w_gate.shape[1] // (2 * LANES)
    plan = Plan(n, rows, chunks)
    parts, blocks = plan.parts, plan.blocks
    own_rows = BLOCK // m
    wire = jnp.bfloat16 if n <= 4 else jnp.float32
    f32, bf16 = jnp.float32, jnp.bfloat16
    hbm = pl.BlockSpec(memory_space=pl.ANY)
    dma = pltpu.SemaphoreType.DMA
    branch, stat = pl.pallas_call(
        functools.partial(kernel, n, m, plan),
        out_shape=[
            jax.ShapeDtypeStruct((rows, width), bf16),
            jax.ShapeDtypeStruct((n * m, 1, rows // m), f32),
        ],
        in_specs=[hbm] * 7,
        out_specs=[hbm] * 2,
        scratch_shapes=[
            pltpu.VMEM((rows, width), bf16),
            pltpu.VMEM((1, width), f32),
            pltpu.VMEM(conv_gate.shape, f32),
            pltpu.VMEM(conv_up.shape, f32),
            pltpu.VMEM((2, chunks, width, 2 * LANES), bf16),
            pltpu.VMEM(w_down.shape, bf16),
            pltpu.VMEM((rows, width), bf16),
            pltpu.VMEM((2, chunks, rows, 2 * LANES), wire),
            pltpu.VMEM((2, chunks, rows, 2 * LANES), wire),
            pltpu.VMEM((rows + 16, 2 * LANES), f32),
            *[pltpu.VMEM((2, rows, (high - low) * LANES), bf16) for low, high, *_ in plan.groups],
            pltpu.VMEM((rows, width), f32),
            pltpu.VMEM((8, rows), f32),
            pltpu.VMEM((2, 8, rows), f32),
            pltpu.VMEM((2, 8, rows), f32),
            pltpu.VMEM((rows + 16, LANES), f32),
            pltpu.VMEM((rows, width), wire),
            pltpu.VMEM((m, blocks, own_rows, width), wire),
            pltpu.VMEM((blocks, own_rows, width), bf16),
            pltpu.VMEM((1, rows // m), f32),
            dma((parts + 3,)), dma((2, 2, chunks)), dma,
            dma((2,)), dma((2, parts, PART // FIRST)), dma((2, chunks, parts)), dma((2, 3)), dma((2, 3, 2 * blocks)),
            dma((2,)), dma((2,)), dma((m,)), dma((blocks, m)), dma((m,)), dma((m,)), dma,
            dma((n, m)), dma((n, m)), dma,
        ],
        compiler_params=pltpu.CompilerParams(
            collective_id=0, has_side_effects=True, vmem_limit_bytes=60 * 1024 * 1024
        ),
    )(tokens[0], pre_gain[None], w_gate, w_up, conv_gate, conv_up, w_down)
    out = pl.pallas_call(
        functools.partial(finish_kernel, n, m),
        out_shape=jax.ShapeDtypeStruct((rows, width), bf16),
        in_specs=[hbm] * 4,
        out_specs=hbm,
        scratch_shapes=[
            pltpu.VMEM((rows, width), bf16),
            pltpu.VMEM((rows, width), bf16),
            pltpu.VMEM((n * m, 1, rows // m), f32),
            pltpu.VMEM((1, width), f32),
            pltpu.VMEM((rows, LANES), f32),
            pltpu.VMEM((rows, width), bf16),
            dma((2 * parts + 2,)), dma((parts,)),
        ],
    )(tokens[0], branch, stat, post_gain[None])
    return out[None]


def solution(mesh):
    in_specs = (
        P("dp", None, "ra"),
        P("ra"),
        P("ra", "cb"),
        P("ra", "cb"),
        P(None, "cb"),
        P(None, "cb"),
        P("cb", "ra"),
        P("ra"),
    )
    out_specs = P("dp", None, "ra")
    return jax.shard_map(
        functools.partial(local, mesh.shape["ra"], mesh.shape["cb"]),
        mesh=mesh, in_specs=in_specs, out_specs=out_specs, check_vma=False,
    )
```

```python
import functools
import jax
import jax.numpy as jnp
from jax import lax
from jax.experimental import pallas as pl
from jax.experimental.pallas import tpu as pltpu
from jax.sharding import PartitionSpec as P

epsilon = 1e-06
residual_scale = 0.125
LANES = 128
PART = 128
BLOCK = 64
STRIPE = 16
LAG = 3
ROW_LAG = 4
LEAD = 5
FIRST = 32
PIECE = 32
MESH = pl.DeviceIdType.MESH


def gelu(v):
    return 0.5 * v * (1.0 + jnp.tanh(0.7978845608028654 * (v + 0.044715 * v * v * v)))


class Plan:
    def __init__(self, n, rows, chunks):
        self.parts = rows // PART
        self.head = self.parts - 1
        self.blocks = rows // BLOCK
        self.upper = chunks * self.head
        self.partials = chunks * self.parts
        self.cut = self.head * PART - PIECE
        self.stripes = rows // STRIPE
        self.early = self.cut // STRIPE
        reach = LAG * (n - 1)
        self.a = max(self.partials, self.upper - 1 + reach)
        self.b = max(self.a + self.early, self.partials - 1 + reach + LEAD)
        self.ring = ROW_LAG * (n - 1) + LEAD + 3
        self.sum_after = 6
        self.slots = self.b + self.stripes - self.early + ROW_LAG * (n - 1) + self.sum_after


def kernel(
    n, m, plan,
    tok_hbm, pre_hbm, wg_hbm, wu_hbm, cg_hbm, cu_hbm, wd_hbm, branch_ref, stat_ref,
    tok, pre, cg, cu,
    w, wd, xw, rbuf, sbuf, full, hid, acc, sq_own, sq_out, sq_in, scale, bsend, brecv, bout, stat,
    lsem, wsem, dsem, psend, pfirst, ring, hsend, sqs, sqr, bss, bsr, oss, osr, osl, sts, str_, stl,
):
    rows, width = tok.shape
    wire = sbuf.dtype
    chunks = w.shape[0]
    half = chunks * LANES
    parts, blocks = plan.parts, plan.blocks
    own_rows = BLOCK // m
    dim_full = width * n
    r = lax.axis_index("ra")
    me = lax.axis_index("cb")
    f32, bf16 = jnp.float32, jnp.bfloat16
    upper = (2 * r) // n

    def place(d):
        return r * (1 - d) + (n - 1 - r) * d

    def onward(d):
        return {"ra": (r + 1 - 2 * d + n) % n}

    def somewhere(i, k):
        return {"ra": (r + i) % n, "cb": (me + k) % m}

    def weight_copies(d, c):
        at = pl.ds(pl.multiple_of(d * half + c * LANES, LANES), LANES)
        return (
            pltpu.make_async_copy(wg_hbm.at[:, at], w.at[c, d, :, pl.ds(0, LANES)], wsem.at[c]),
            pltpu.make_async_copy(wu_hbm.at[:, at], w.at[c, d, :, pl.ds(LANES, LANES)], wsem.at[c]),
        )

    tok_copies = [
        pltpu.make_async_copy(tok_hbm.at[pl.ds(q * PART, PART)], tok.at[pl.ds(q * PART, PART)], lsem.at[q])
        for q in range(parts)
    ]
    pre_copy = pltpu.make_async_copy(pre_hbm, pre, lsem.at[parts])
    rest = [
        pltpu.make_async_copy(cg_hbm, cg, lsem.at[parts + 1]),
        pltpu.make_async_copy(cu_hbm, cu, lsem.at[parts + 2]),
    ]
    pre_copy.start()
    tok_copies[0].start()
    for d in (0, 1):
        for copy in weight_copies(d, 0):
            copy.start()
    for copy in tok_copies[1:]:
        copy.start()

    barrier = pltpu.get_barrier_semaphore()
    others = [(i, k) for k in range(m) for i in range(n) if i or k]

    for d in (0, 1):
        @pl.when(place(d) < n - 1)
        def _():
            pl.semaphore_signal(barrier, inc=1, device_id=onward(d), device_id_type=MESH)

    for k in range(1, m):
        pl.semaphore_signal(barrier, inc=1, device_id=somewhere(0, k), device_id_type=MESH)

    for copy in rest:
        copy.start()

    down_copy = pltpu.make_async_copy(wd_hbm, wd, dsem)

    def fetch(c):
        for d in (0, 1):
            for copy in weight_copies(d, c):
                copy.start()

    fetch(1)
    for c in range(chunks):
        full[c, pl.ds(0, 8), :] = jnp.zeros((8, 2 * LANES), f32)
        full[c, pl.ds(rows + 8, 8), :] = jnp.zeros((8, 2 * LANES), f32)
    scale[pl.ds(0, 8), :] = jnp.zeros((8, LANES), f32)
    scale[pl.ds(rows + 8, 8), :] = jnp.zeros((8, LANES), f32)

    def square_copy(d):
        return pltpu.make_async_remote_copy(
            src_ref=sq_out.at[d], dst_ref=sq_in.at[d],
            send_sem=sqs.at[d], recv_sem=sqr.at[d],
            device_id=onward(d), device_id_type=MESH,
        )

    def own_squares():
        values = tok[...].astype(f32)
        square = values * values
        high = square.astype(bf16)
        low = (square - high.astype(f32)).astype(bf16)
        ones = jnp.ones((8, width), bf16)
        nt = (((1,), (1,)), ((), ()))
        sq_own[...] = lax.dot_general(ones, high, nt, preferred_element_type=f32) + lax.dot_general(
            ones, low, nt, preferred_element_type=f32
        )

    def square_step(d):
        p = place(d)

        @pl.when(p == 0)
        def _():
            sq_out[d] = sq_own[...]

        @pl.when(p > 0)
        def _():
            square_copy(d).wait_recv()
            sq_out[d] = sq_own[...] + sq_in[d]

        @pl.when(p < n - 1)
        def _():
            square_copy(d).start()

        @pl.when(p == n - 1)
        def _():
            inv = lax.rsqrt(sq_out[d] / dim_full + epsilon)
            scale[pl.ds(8, rows), :] = jnp.concatenate([inv] * (LANES // 8), axis=0).T

    def part_rows(b):
        return pl.ds(pl.multiple_of(b * PART, PART), PART)

    def block_rows(b):
        return pl.ds(pl.multiple_of(b * BLOCK, BLOCK), BLOCK)

    def partial_copy(d, i, c, b):
        at = part_rows(b)
        return pltpu.make_async_remote_copy(
            src_ref=sbuf.at[d, c, at], dst_ref=rbuf.at[d, c, at],
            send_sem=psend.at[d], recv_sem=ring.at[d, i % plan.ring],
            device_id=onward(d), device_id_type=MESH,
        )

    def first_copy(d, j):
        at = pl.ds(j * FIRST, FIRST)
        return pltpu.make_async_remote_copy(
            src_ref=sbuf.at[d, 0, at], dst_ref=rbuf.at[d, 0, at],
            send_sem=psend.at[d], recv_sem=pfirst.at[d, j],
            device_id=onward(d), device_id_type=MESH,
        )

    def hidden_copy(d, k):
        at = pl.ds(pl.multiple_of(k * STRIPE, STRIPE), STRIPE)
        return pltpu.make_async_remote_copy(
            src_ref=hid.at[1 - d, at], dst_ref=hid.at[1 - d, at],
            send_sem=hsend.at[d], recv_sem=ring.at[d, (plan.partials + k) % plan.ring],
            device_id=onward(d), device_id_type=MESH,
        )

    def finish_rows(d, c, low, high):
        at = pl.ds(pl.multiple_of(d * half + c * LANES, LANES), LANES)
        to = pl.ds(pl.multiple_of(c * LANES, LANES), LANES)
        taps_g, taps_u = cg[:, at], cu[:, at]
        for j in range(low, high, PIECE):
            by = scale[pl.ds(j, PIECE + 16), :]
            window = full[c, pl.ds(j, PIECE + 16), :] * jnp.concatenate([by, by], axis=1)
            before = pltpu.roll(window, 1, 0)[8:8 + PIECE]
            here = window[8:8 + PIECE]
            after = pltpu.roll(window, PIECE + 15, 0)[8:8 + PIECE]
            conv = []
            for side, taps in ((0, taps_g), (1, taps_u)):
                lanes = slice(side * LANES, (side + 1) * LANES)
                conv.append(
                    taps[0:1] * before[:, lanes] + taps[1:2] * here[:, lanes] + taps[2:3] * after[:, lanes]
                )
            hid[d, pl.ds(j, PIECE), to] = (gelu(conv[0]) * conv[1]).astype(bf16)

    def partial_step(d, i):
        p = place(d)
        c = jnp.where(i < plan.upper, i // plan.head, i - plan.upper)
        b = jnp.where(i < plan.upper, i % plan.head, plan.head)
        at = part_rows(b)
        own = jnp.dot(xw[at, :], w[c, d], preferred_element_type=f32)

        @pl.when((p < n - 1) & (i == 0))
        def _():
            for j in range(PART // FIRST):
                some = pl.ds(j * FIRST, FIRST)
                piece = own[j * FIRST:(j + 1) * FIRST]

                @pl.when(p == 0)
                def _():
                    sbuf[d, 0, some] = piece.astype(wire)

                @pl.when(p > 0)
                def _():
                    first_copy(d, j).wait_recv()
                    sbuf[d, 0, some] = (piece + rbuf[d, 0, some].astype(f32)).astype(wire)

                first_copy(d, j).start()

        @pl.when((p == 0) & (i > 0))
        def _():
            sbuf[d, c, at] = own.astype(wire)
            partial_copy(d, i, c, b).start()

        @pl.when((p > 0) & (p < n - 1) & (i > 0))
        def _():
            partial_copy(d, i, c, b).wait_recv()
            sbuf[d, c, at] = (own + rbuf[d, c, at].astype(f32)).astype(wire)
            partial_copy(d, i, c, b).start()

        @pl.when(p == n - 1)
        def _():
            @pl.when(i == 0)
            def _():
                for j in range(PART // FIRST):
                    first_copy(d, j).wait_recv()

            @pl.when(i > 0)
            def _():
                partial_copy(d, i, c, b).wait_recv()

            full[c, pl.ds(pl.multiple_of(b * PART + 8, 8), PART), :] = own + rbuf[d, c, at].astype(f32)

            @pl.when(b == plan.head - 1)
            def _():
                finish_rows(d, c, 0, plan.cut)

            @pl.when(b == plan.head)
            def _():
                finish_rows(d, c, plan.cut, rows)

    def hidden_pass(d, k):
        p = place(d)

        @pl.when(p > 0)
        def _():
            hidden_copy(d, k).wait_recv()

        @pl.when((p > 0) & (p < n - 1))
        def _():
            hidden_copy(d, k).start()

    def hidden_use(d, k):
        every = BLOCK // STRIPE

        @pl.when(k % every == every - 1)
        def _():
            at = block_rows(k // every)
            acc[at, :] += jnp.dot(
                hid[1 - d, at, :], wd[pl.ds(pl.multiple_of((1 - d) * half, LANES), half), :],
                preferred_element_type=f32,
            )

    def mine(b):
        return pl.ds(pl.multiple_of(b * BLOCK + me * own_rows, own_rows), own_rows)

    def branch_copy(b, k):
        peer = (me + k) % m
        at = pl.ds(pl.multiple_of(b * BLOCK + peer * own_rows, own_rows), own_rows)
        return pltpu.make_async_remote_copy(
            src_ref=bsend.at[at], dst_ref=brecv.at[b, k],
            send_sem=bss.at[k], recv_sem=bsr.at[b],
            device_id={"cb": peer}, device_id_type=MESH,
        )

    def out_copy(b, k):
        return pltpu.make_async_remote_copy(
            src_ref=bout.at[b], dst_ref=branch_ref.at[mine(b)],
            send_sem=oss.at[k], recv_sem=osr.at[k],
            device_id={"cb": (me + k) % m}, device_id_type=MESH,
        )

    def stat_copy(i, k):
        return pltpu.make_async_remote_copy(
            src_ref=stat, dst_ref=stat_ref.at[r * m + me],
            send_sem=sts, recv_sem=str_,
            device_id=somewhere(i, k), device_id_type=MESH,
        )

    keep_stat = pltpu.make_async_copy(stat, stat_ref.at[r * m + me], stl)

    def send_branch(b):
        at = block_rows(b)
        bsend[at, :] = acc[at, :].astype(wire)
        for k in range(1, m):
            branch_copy(b, k).start()

    def sum_branch(b):
        branch = acc[mine(b), :]
        incoming = brecv.at[b, pl.ds(1, m - 1)]
        pltpu.make_async_copy(incoming, incoming, bsr.at[b]).wait()
        for k in range(1, m):
            branch = branch + brecv[b, k].astype(f32)
        bout[b] = branch.astype(bf16)
        for k in range(1, m):
            out_copy(b, k).start()
        pltpu.make_async_copy(bout.at[b], branch_ref.at[mine(b)], osl).start()
        sums = jnp.sum(branch * branch, axis=1, keepdims=True)
        lanes = stat.shape[1]
        lane = lax.broadcasted_iota(jnp.int32, (own_rows, lanes), 1)
        row = lax.broadcasted_iota(jnp.int32, (own_rows, lanes), 0)
        spread = jnp.sum(jnp.where(lane == b * own_rows + row, sums, 0.0), axis=0, keepdims=True)
        stat[...] = stat[...] + spread

        @pl.when(b == blocks - 1)
        def _():
            for i, k in others:
                stat_copy(i, k).start()
            keep_stat.start()

    pre_copy.wait()

    def slot(s, carry):
        def take(q):
            at = part_rows(q)
            pltpu.make_async_copy(tok_hbm.at[at], tok.at[at], lsem.at[q]).wait()
            xw[at, :] = (tok[at, :].astype(f32) * pre[...]).astype(bf16)

        @pl.when(s < plan.head)
        def _():
            take(jnp.minimum(s, parts - 1))

        @pl.when(s == 0)
        def _():
            pl.semaphore_wait(barrier, jnp.where((r == 0) | (r == n - 1), 1, 2) + m - 1)

        @pl.when(s == plan.head - 1)
        def _():
            take(plan.head)
            for copy in rest:
                copy.wait()
            own_squares()

        t = s - LAG * jnp.minimum(r, n - 1 - r)

        @pl.when((t >= 0) & (t < plan.upper) & (t % plan.head == 0))
        def _():
            c = t // plan.head
            pltpu.make_async_copy(w.at[c], w.at[c], wsem.at[c]).wait()

        for order in (0, 1):
            d = (order + 1 - upper) % 2
            i = s - LAG * place(d)

            @pl.when(i == plan.head - 1)
            def _():
                square_step(d)

            @pl.when((i >= 0) & (i < plan.partials))
            def _():
                partial_step(d, i)

        @pl.when((s >= 1) & (s < chunks - 1))
        def _():
            fetch(s + 1)

        @pl.when(s == chunks)
        def _():
            down_copy.start()
            acc[...] = jnp.zeros_like(acc)
            stat[...] = jnp.zeros_like(stat)

        @pl.when(s == plan.partials)
        def _():
            down_copy.wait()

        for order in (0, 1):
            d = (order + 1 - upper) % 2
            p = place(d)

            @pl.when((p == 0) & (s == plan.a))
            def _():
                def send(j, carry):
                    hidden_copy(d, j).start()
                    return carry

                lax.fori_loop(0, LEAD, send, 0)

            ahead = s + LEAD - plan.a

            @pl.when((p == 0) & (s >= plan.a) & (ahead < plan.early))
            def _():
                hidden_copy(d, ahead).start()

            ahead = s + LEAD - plan.b

            @pl.when((p == 0) & (ahead >= 0) & (ahead < plan.stripes - plan.early))
            def _():
                hidden_copy(d, ahead + plan.early).start()

        def stripe(t):
            k = jnp.where(t < plan.b, t - plan.a, t - plan.b + plan.early)
            return k, ((t >= plan.a) & (t < plan.a + plan.early)) | ((t >= plan.b) & (k < plan.stripes))

        for step in (hidden_pass, hidden_use):
            for order in (0, 1):
                d = (order + 1 - upper) % 2
                k, live = stripe(s - ROW_LAG * place(d))

                @pl.when(live)
                def _():
                    step(d, k)

        every = BLOCK // STRIPE
        done = s - ROW_LAG * jnp.maximum(r, n - 1 - r)
        send_at, live = stripe(done)

        @pl.when(live & (send_at % every == every - 1))
        def _():
            send_branch(send_at // every)

        sum_at, live = stripe(done - plan.sum_after)

        @pl.when(live & (sum_at % every == every - 1))
        def _():
            sum_branch(sum_at // every)

        return carry

    lax.fori_loop(0, plan.slots, slot, 0)

    for d in (0, 1):
        @pl.when(place(d) < n - 1)
        def _():
            square_copy(d).wait_send()
            for buffer, sem in ((sbuf.at[d], psend.at[d]), (hid.at[1 - d], hsend.at[d])):
                pltpu.make_async_remote_copy(
                    src_ref=buffer, dst_ref=buffer, send_sem=sem, recv_sem=ring.at[d, 0],
                    device_id=onward(d), device_id_type=MESH,
                ).wait_send()

    for k in range(1, m):
        peer = {"cb": (me + k) % m}
        sent = brecv.at[:, k]
        pltpu.make_async_remote_copy(
            src_ref=sent, dst_ref=sent, send_sem=bss.at[k], recv_sem=bsr.at[0],
            device_id=peer, device_id_type=MESH,
        ).wait_send()
        share = branch_ref.at[pl.ds(0, rows // m)]
        pltpu.make_async_remote_copy(
            src_ref=bout, dst_ref=bout, send_sem=oss.at[k], recv_sem=osr.at[k],
            device_id=peer, device_id_type=MESH,
        ).wait_send()
        pltpu.make_async_remote_copy(
            src_ref=share, dst_ref=share, send_sem=oss.at[k], recv_sem=osr.at[k],
            device_id=peer, device_id_type=MESH,
        ).wait_recv()
    share = branch_ref.at[pl.ds(0, rows // m)]
    pltpu.make_async_copy(share, share, osl).wait()
    all_stats = stat_ref.at[pl.ds(0, len(others))]
    both = pltpu.make_async_remote_copy(
        src_ref=all_stats, dst_ref=all_stats, send_sem=sts, recv_sem=str_,
        device_id=somewhere(0, 1), device_id_type=MESH,
    )
    both.wait_send()
    both.wait_recv()
    keep_stat.wait()


def finish_kernel(
    n, m, tok_hbm, branch_hbm, stat_hbm, post_hbm, out_hbm,
    tok, branch, stat, post, scale, out, isem, osem,
):
    rows, width = tok.shape
    parts = rows // PART
    blocks = rows // BLOCK
    own_rows = BLOCK // m
    f32 = jnp.float32
    stat_copy = pltpu.make_async_copy(stat_hbm, stat, isem.at[2 * parts])
    post_copy = pltpu.make_async_copy(post_hbm, post, isem.at[2 * parts + 1])
    stat_copy.start()
    post_copy.start()
    copies = []
    for q in range(parts):
        at = pl.ds(q * PART, PART)
        pair = (
            pltpu.make_async_copy(branch_hbm.at[at], branch.at[at], isem.at[q]),
            pltpu.make_async_copy(tok_hbm.at[at], tok.at[at], isem.at[parts + q]),
        )
        for copy in pair:
            copy.start()
        copies.append(pair)
    stat_copy.wait()
    for k in range(m):
        total = stat[k]
        for i in range(1, n):
            total = total + stat[i * m + k]
        inv = lax.rsqrt(total / (width * n) + epsilon)
        column = jnp.broadcast_to(inv, (LANES, rows // m)).T
        for b in range(blocks):
            scale[pl.ds(b * BLOCK + k * own_rows, own_rows), :] = column[b * own_rows:(b + 1) * own_rows]
    post_copy.wait()
    writes = []
    for q in range(parts):
        for copy in copies[q]:
            copy.wait()
        at = pl.ds(q * PART, PART)
        by = scale[at, :]
        for t in range(width // LANES):
            lanes = pl.ds(t * LANES, LANES)
            mixed = residual_scale * tok[at, lanes].astype(f32) + branch[at, lanes].astype(f32) * by * post[:, lanes]
            out[at, lanes] = mixed.astype(out.dtype)
        write = pltpu.make_async_copy(out.at[at], out_hbm.at[at], osem.at[q])
        write.start()
        writes.append(write)
    for write in writes:
        write.wait()


def local(n, m, tokens, pre_gain, w_gate, w_up, conv_gate, conv_up, w_down, post_gain):
    rows, width = tokens.shape[1:]
    chunks = w_gate.shape[1] // (2 * LANES)
    plan = Plan(n, rows, chunks)
    parts, blocks = plan.parts, plan.blocks
    own_rows = BLOCK // m
    wire = jnp.bfloat16 if n <= 4 else jnp.float32
    f32, bf16 = jnp.float32, jnp.bfloat16
    hbm = pl.BlockSpec(memory_space=pl.ANY)
    dma = pltpu.SemaphoreType.DMA
    branch, stat = pl.pallas_call(
        functools.partial(kernel, n, m, plan),
        out_shape=[
            jax.ShapeDtypeStruct((rows, width), bf16),
            jax.ShapeDtypeStruct((n * m, 1, rows // m), f32),
        ],
        in_specs=[hbm] * 7,
        out_specs=[hbm] * 2,
        scratch_shapes=[
            pltpu.VMEM((rows, width), bf16),
            pltpu.VMEM((1, width), f32),
            pltpu.VMEM(conv_gate.shape, f32),
            pltpu.VMEM(conv_up.shape, f32),
            pltpu.VMEM((chunks, 2, width, 2 * LANES), bf16),
            pltpu.VMEM(w_down.shape, bf16),
            pltpu.VMEM((rows, width), bf16),
            pltpu.VMEM((2, chunks, rows, 2 * LANES), wire),
            pltpu.VMEM((2, chunks, rows, 2 * LANES), wire),
            pltpu.VMEM((chunks, rows + 16, 2 * LANES), f32),
            pltpu.VMEM((2, rows, chunks * LANES), bf16),
            pltpu.VMEM((rows, width), f32),
            pltpu.VMEM((8, rows), f32),
            pltpu.VMEM((2, 8, rows), f32),
            pltpu.VMEM((2, 8, rows), f32),
            pltpu.VMEM((rows + 16, LANES), f32),
            pltpu.VMEM((rows, width), wire),
            pltpu.VMEM((blocks, m, own_rows, width), wire),
            pltpu.VMEM((blocks, own_rows, width), bf16),
            pltpu.VMEM((1, rows // m), f32),
            dma((parts + 3,)), dma((chunks,)), dma,
            dma((2,)), dma((2, PART // FIRST)), dma((2, plan.ring)), dma((2,)),
            dma((2,)), dma((2,)), dma((m,)), dma((blocks,)), dma((m,)), dma((m,)), dma,
            dma, dma, dma,
        ],
        compiler_params=pltpu.CompilerParams(
            collective_id=0, has_side_effects=True, vmem_limit_bytes=60 * 1024 * 1024
        ),
    )(tokens[0], pre_gain[None], w_gate, w_up, conv_gate, conv_up, w_down)
    out = pl.pallas_call(
        functools.partial(finish_kernel, n, m),
        out_shape=jax.ShapeDtypeStruct((rows, width), bf16),
        in_specs=[hbm] * 4,
        out_specs=hbm,
        scratch_shapes=[
            pltpu.VMEM((rows, width), bf16),
            pltpu.VMEM((rows, width), bf16),
            pltpu.VMEM((n * m, 1, rows // m), f32),
            pltpu.VMEM((1, width), f32),
            pltpu.VMEM((rows, LANES), f32),
            pltpu.VMEM((rows, width), bf16),
            dma((2 * parts + 2,)), dma((parts,)),
        ],
    )(tokens[0], branch, stat, post_gain[None])
    return out[None]


def solution(mesh):
    in_specs = (
        P("dp", None, "ra"),
        P("ra"),
        P("ra", "cb"),
        P("ra", "cb"),
        P(None, "cb"),
        P(None, "cb"),
        P("cb", "ra"),
        P("ra"),
    )
    out_specs = P("dp", None, "ra")
    return jax.shard_map(
        functools.partial(local, mesh.shape["ra"], mesh.shape["cb"]),
        mesh=mesh, in_specs=in_specs, out_specs=out_specs, check_vma=False,
    )
```

```python
import functools
import jax
import jax.numpy as jnp
from jax import lax
from jax.experimental import pallas as pl
from jax.experimental.pallas import tpu as pltpu
from jax.sharding import PartitionSpec as P

epsilon = 1e-06
residual_scale = 0.125
LANES = 128
PART = 128
BLOCK = 64
STRIPE = 16
LAG = 3
ROW_LAG = 4
LEAD = 5
FIRST = 32
PIECE = 32
MESH = pl.DeviceIdType.MESH


def gelu(v):
    return 0.5 * v * (1.0 + jnp.tanh(0.7978845608028654 * (v + 0.044715 * v * v * v)))


class Plan:
    def __init__(self, n, rows, chunks):
        self.parts = rows // PART
        self.head = self.parts - 1
        self.blocks = rows // BLOCK - 1
        self.upper = chunks * self.head
        self.partials = chunks * self.parts
        self.cut = self.head * PART - PIECE
        self.stripes = rows // STRIPE
        self.early = self.cut // STRIPE
        reach = LAG * (n - 1)
        self.a = max(self.partials, self.upper - 1 + reach)
        self.b = max(self.a + self.early, self.partials - 1 + reach + LEAD)
        self.ring = ROW_LAG * (n - 1) + LEAD + 3
        self.sum_after = 5
        self.tail = max(self.a, self.partials + reach)
        self.slots = self.b + self.stripes - self.early + ROW_LAG * (n - 1)


def kernel(
    n, m, plan,
    tok_hbm, pre_hbm, wg_hbm, wu_hbm, cg_hbm, cu_hbm, wd_hbm, branch_ref, stat_ref,
    tok, pre, cg, cu,
    w, wd, xw, rbuf, sbuf, full, hid, acc, sq_own, sq_out, sq_in, scale, bsend, brecv, bout, hsend_rows, hrecv_rows, hout, stat,
    lsem, wsem, dsem, psend, pfirst, ring, hsend, sqs, sqr, bss, bsr, oss, osr, osl, hss, hsr, hos, sts, str_, stl,
):
    rows, width = tok.shape
    wire = sbuf.dtype
    chunks = w.shape[0]
    half = chunks * LANES
    parts, blocks = plan.parts, plan.blocks
    own_rows = BLOCK // m
    half_own = own_rows // 2
    dim_full = width * n
    r = lax.axis_index("ra")
    me = lax.axis_index("cb")
    f32, bf16 = jnp.float32, jnp.bfloat16
    upper = (2 * r) // n

    def place(d):
        return r * (1 - d) + (n - 1 - r) * d

    def onward(d):
        return {"ra": (r + 1 - 2 * d + n) % n}

    def somewhere(i, k):
        return {"ra": (r + i) % n, "cb": (me + k) % m}

    def weight_copies(d, c):
        at = pl.ds(pl.multiple_of(d * half + c * LANES, LANES), LANES)
        return (
            pltpu.make_async_copy(wg_hbm.at[:, at], w.at[c, d, :, pl.ds(0, LANES)], wsem.at[lax.rem(c, 4)]),
            pltpu.make_async_copy(wu_hbm.at[:, at], w.at[c, d, :, pl.ds(LANES, LANES)], wsem.at[lax.rem(c, 4)]),
        )

    tok_copies = [
        pltpu.make_async_copy(tok_hbm.at[pl.ds(q * PART, PART)], tok.at[pl.ds(q * PART, PART)], lsem.at[q])
        for q in range(parts)
    ]
    pre_copy = pltpu.make_async_copy(pre_hbm, pre, lsem.at[parts])
    rest = [
        pltpu.make_async_copy(cg_hbm, cg, lsem.at[parts + 1]),
        pltpu.make_async_copy(cu_hbm, cu, lsem.at[parts + 2]),
    ]
    pre_copy.start()
    tok_copies[0].start()
    for d in (0, 1):
        for copy in weight_copies(d, 0):
            copy.start()
    for copy in tok_copies[1:]:
        copy.start()

    barrier = pltpu.get_barrier_semaphore()
    others = [(i, k) for k in range(m) for i in range(n) if i or k]

    for d in (0, 1):
        @pl.when(place(d) < n - 1)
        def _():
            pl.semaphore_signal(barrier, inc=1, device_id=onward(d), device_id_type=MESH)

    for k in range(1, m):
        pl.semaphore_signal(barrier, inc=1, device_id=somewhere(0, k), device_id_type=MESH)

    down_copy = pltpu.make_async_copy(wd_hbm, wd, dsem)

    def fetch(c):
        for d in (0, 1):
            for copy in weight_copies(d, c):
                copy.start()

    def square_copy(d):
        return pltpu.make_async_remote_copy(
            src_ref=sq_out.at[d], dst_ref=sq_in.at[d],
            send_sem=sqs.at[d], recv_sem=sqr.at[d],
            device_id=onward(d), device_id_type=MESH,
        )

    def own_squares():
        values = tok[...].astype(f32)
        square = values * values
        high = square.astype(bf16)
        low = (square - high.astype(f32)).astype(bf16)
        ones = jnp.ones((8, width), bf16)
        nt = (((1,), (1,)), ((), ()))
        sq_own[...] = lax.dot_general(ones, high, nt, preferred_element_type=f32) + lax.dot_general(
            ones, low, nt, preferred_element_type=f32
        )

    def square_step(d):
        p = place(d)

        @pl.when(p == 0)
        def _():
            sq_out[d] = sq_own[...]

        @pl.when(p > 0)
        def _():
            square_copy(d).wait_recv()
            sq_out[d] = sq_own[...] + sq_in[d]

        @pl.when(p < n - 1)
        def _():
            square_copy(d).start()

        @pl.when(p == n - 1)
        def _():
            inv = lax.rsqrt(sq_out[d] / dim_full + epsilon)
            scale[pl.ds(8, rows), :] = jnp.concatenate([inv] * (LANES // 8), axis=0).T

    def part_rows(b):
        return pl.ds(pl.multiple_of(b * PART, PART), PART)

    def block_rows(b):
        return pl.ds(pl.multiple_of(b * BLOCK, BLOCK), BLOCK)

    def partial_copy(d, i, c, b):
        at = part_rows(b)
        return pltpu.make_async_remote_copy(
            src_ref=sbuf.at[d, c, at], dst_ref=rbuf.at[d, c, at],
            send_sem=psend.at[d], recv_sem=ring.at[d, lax.rem(i, plan.ring)],
            device_id=onward(d), device_id_type=MESH,
        )

    def first_copy(d, j):
        at = pl.ds(j * FIRST, FIRST)
        return pltpu.make_async_remote_copy(
            src_ref=sbuf.at[d, 0, at], dst_ref=rbuf.at[d, 0, at],
            send_sem=psend.at[d], recv_sem=pfirst.at[d, j],
            device_id=onward(d), device_id_type=MESH,
        )

    def hidden_copy(d, k):
        at = pl.ds(pl.multiple_of(k * STRIPE, STRIPE), STRIPE)
        return pltpu.make_async_remote_copy(
            src_ref=hid.at[1 - d, at], dst_ref=hid.at[1 - d, at],
            send_sem=hsend.at[d], recv_sem=ring.at[d, lax.rem(plan.partials + k, plan.ring)],
            device_id=onward(d), device_id_type=MESH,
        )

    def finish_rows(d, c, low, high):
        at = pl.ds(pl.multiple_of(d * half + c * LANES, LANES), LANES)
        to = pl.ds(pl.multiple_of(c * LANES, LANES), LANES)
        taps_g, taps_u = cg[:, at], cu[:, at]
        for j in range(low, high, PIECE):
            by = scale[pl.ds(j, PIECE + 16), :]
            window = full[c, pl.ds(j, PIECE + 16), :] * jnp.concatenate([by, by], axis=1)
            before = pltpu.roll(window, 1, 0)[8:8 + PIECE]
            here = window[8:8 + PIECE]
            after = pltpu.roll(window, PIECE + 15, 0)[8:8 + PIECE]
            conv = []
            for side, taps in ((0, taps_g), (1, taps_u)):
                lanes = slice(side * LANES, (side + 1) * LANES)
                conv.append(
                    taps[0:1] * before[:, lanes] + taps[1:2] * here[:, lanes] + taps[2:3] * after[:, lanes]
                )
            hid[d, pl.ds(j, PIECE), to] = (gelu(conv[0]) * conv[1]).astype(bf16)

    def partial_step(d, i):
        p = place(d)
        c = jnp.where(i < plan.upper, lax.div(i, plan.head), i - plan.upper)
        b = jnp.where(i < plan.upper, lax.rem(i, plan.head), plan.head)
        at = part_rows(b)
        own = jnp.dot(xw[at, :], w[c, d], preferred_element_type=f32)

        @pl.when((p < n - 1) & (i == 0))
        def _():
            for j in range(PART // FIRST):
                some = pl.ds(j * FIRST, FIRST)
                piece = own[j * FIRST:(j + 1) * FIRST]

                @pl.when(p == 0)
                def _():
                    sbuf[d, 0, some] = piece.astype(wire)

                @pl.when(p > 0)
                def _():
                    first_copy(d, j).wait_recv()
                    sbuf[d, 0, some] = (piece + rbuf[d, 0, some].astype(f32)).astype(wire)

                first_copy(d, j).start()

        @pl.when((p == 0) & (i > 0))
        def _():
            sbuf[d, c, at] = own.astype(wire)
            partial_copy(d, i, c, b).start()

        @pl.when((p > 0) & (p < n - 1) & (i > 0))
        def _():
            partial_copy(d, i, c, b).wait_recv()
            sbuf[d, c, at] = (own + rbuf[d, c, at].astype(f32)).astype(wire)
            partial_copy(d, i, c, b).start()

        @pl.when(p == n - 1)
        def _():
            @pl.when(i == 0)
            def _():
                for j in range(PART // FIRST):
                    first_copy(d, j).wait_recv()

            @pl.when(i > 0)
            def _():
                partial_copy(d, i, c, b).wait_recv()

            full[c, pl.ds(pl.multiple_of(b * PART + 8, 8), PART), :] = own + rbuf[d, c, at].astype(f32)

            @pl.when(b == plan.head - 1)
            def _():
                finish_rows(d, c, 0, plan.cut)

            @pl.when(b == plan.head)
            def _():
                finish_rows(d, c, plan.cut, rows)

    def hidden_pass(d, k):
        p = place(d)

        @pl.when(p > 0)
        def _():
            hidden_copy(d, k).wait_recv()

        @pl.when((p > 0) & (p < n - 1))
        def _():
            hidden_copy(d, k).start()

    def hidden_use(d, k):
        every = BLOCK // STRIPE

        def product(at):
            acc[at, :] += jnp.dot(
                hid[1 - d, at, :], wd[pl.ds(pl.multiple_of((1 - d) * half, LANES), half), :],
                preferred_element_type=f32,
            )

        @pl.when((lax.rem(k, every) == every - 1) & (k < plan.stripes - every))
        def _():
            product(block_rows(lax.div(k, every)))

        ends = place(d) == n - 1

        @pl.when((k == plan.stripes - 1) & jnp.logical_not(ends))
        def _():
            product(pl.ds(rows - BLOCK, BLOCK))

        for h in (0, 1):
            @pl.when((k == plan.stripes - 1 - (1 - h) * every // 2) & ends)
            def _():
                product(pl.ds(rows - BLOCK + h * BLOCK // 2, BLOCK // 2))

    def mine(b):
        return pl.ds(pl.multiple_of(b * BLOCK + me * own_rows, own_rows), own_rows)

    def branch_copy(b, k):
        peer = (me + k) % m
        at = pl.ds(pl.multiple_of(b * BLOCK + peer * own_rows, own_rows), own_rows)
        return pltpu.make_async_remote_copy(
            src_ref=bsend.at[at], dst_ref=brecv.at[b, k],
            send_sem=bss.at[k - 1], recv_sem=bsr.at[b],
            device_id={"cb": peer}, device_id_type=MESH,
        )

    def out_copy(b, k):
        return pltpu.make_async_remote_copy(
            src_ref=bout.at[b], dst_ref=branch_ref.at[mine(b)],
            send_sem=oss.at[k - 1], recv_sem=osr.at[k - 1],
            device_id={"cb": (me + k) % m}, device_id_type=MESH,
        )

    def stat_copy(i, k):
        return pltpu.make_async_remote_copy(
            src_ref=stat, dst_ref=stat_ref.at[r * m + me],
            send_sem=sts, recv_sem=str_,
            device_id=somewhere(i, k), device_id_type=MESH,
        )

    keep_stat = pltpu.make_async_copy(stat, stat_ref.at[r * m + me], stl)

    def send_branch(b):
        at = block_rows(b)
        bsend[at, :] = acc[at, :].astype(wire)
        for k in range(1, m):
            branch_copy(b, k).start()

    def half_row(h, peer):
        return pl.ds(pl.multiple_of(rows - BLOCK + h * (BLOCK // 2) + peer * half_own, half_own), half_own)

    def half_copy(h, k):
        return pltpu.make_async_remote_copy(
            src_ref=hsend_rows.at[h, (me + k) % m], dst_ref=hrecv_rows.at[h, k],
            send_sem=hss.at[k - 1], recv_sem=hsr.at[h],
            device_id={"cb": (me + k) % m}, device_id_type=MESH,
        )

    def half_out(h, k):
        return pltpu.make_async_remote_copy(
            src_ref=hout.at[h], dst_ref=branch_ref.at[half_row(h, me)],
            send_sem=hos.at[k - 1], recv_sem=osr.at[k - 1],
            device_id={"cb": (me + k) % m}, device_id_type=MESH,
        )

    def keep_half(h):
        return pltpu.make_async_copy(hout.at[h], branch_ref.at[half_row(h, me)], osl)

    def send_half(h):
        for peer in range(m):
            hsend_rows[h, peer] = acc[half_row(h, peer), :].astype(wire)
        for k in range(1, m):
            half_copy(h, k).start()

    def add_stat(branch, first):
        sums = jnp.sum(branch * branch, axis=1, keepdims=True)
        shape = (branch.shape[0], stat.shape[1])
        lane = lax.broadcasted_iota(jnp.int32, shape, 1)
        row = lax.broadcasted_iota(jnp.int32, shape, 0)
        spread = jnp.sum(jnp.where(lane == first + row, sums, 0.0), axis=0, keepdims=True)
        stat[...] = stat[...] + spread

    def sum_half(h):
        incoming = hrecv_rows.at[h, pl.ds(1, m - 1)]
        pltpu.make_async_copy(incoming, incoming, hsr.at[h]).wait()
        branch = acc[half_row(h, me), :]
        for k in range(1, m):
            branch = branch + hrecv_rows[h, k].astype(f32)
        add_stat(branch, rows // m - own_rows + h * half_own)
        if h:
            for i, k in others:
                stat_copy(i, k).start()
            keep_stat.start()
        hout[h] = branch.astype(bf16)
        for k in range(1, m):
            half_out(h, k).start()
        keep_half(h).start()

    def sum_branch(b):
        branch = acc[mine(b), :]
        incoming = brecv.at[b, pl.ds(1, m - 1)]
        pltpu.make_async_copy(incoming, incoming, bsr.at[b]).wait()
        for k in range(1, m):
            branch = branch + brecv[b, k].astype(f32)
        bout[b] = branch.astype(bf16)
        for k in range(1, m):
            out_copy(b, k).start()
        pltpu.make_async_copy(bout.at[b], branch_ref.at[mine(b)], osl).start()
        add_stat(branch, b * own_rows)

    pre_copy.wait()

    def partial_slot(s):
        def take(q):
            at = part_rows(q)
            pltpu.make_async_copy(tok_hbm.at[at], tok.at[at], lsem.at[q]).wait()
            xw[at, :] = (tok[at, :].astype(f32) * pre[...]).astype(bf16)

        @pl.when(s < plan.head)
        def _():
            take(jnp.minimum(s, parts - 1))

        @pl.when(s == 0)
        def _():
            pl.semaphore_wait(barrier, jnp.where((r == 0) | (r == n - 1), 1, 2) + m - 1)

        @pl.when(s == plan.head - 1)
        def _():
            take(plan.head)
            for copy in rest:
                copy.wait()
            own_squares()

        t = s - LAG * jnp.minimum(r, n - 1 - r)

        @pl.when((t >= 0) & (t < plan.upper) & (lax.rem(t, plan.head) == 0))
        def _():
            c = lax.div(t, plan.head)
            pltpu.make_async_copy(w.at[c], w.at[c], wsem.at[lax.rem(c, 4)]).wait()

            @pl.when(c + 3 < chunks)
            def _():
                fetch(c + 3)

        for order in (0, 1):
            d = (order + 1 - upper) % 2
            i = s - LAG * place(d)

            @pl.when(i == plan.head - 1)
            def _():
                square_step(d)

            @pl.when((i >= 0) & (i < plan.partials))
            def _():
                partial_step(d, i)

        @pl.when(s == 0)
        def _():
            for copy in rest:
                copy.start()
            for at in (0, rows + 8):
                scale[pl.ds(at, 8), :] = jnp.zeros((8, LANES), f32)
                for c in range(chunks):
                    full[c, pl.ds(at, 8), :] = jnp.zeros((8, 2 * LANES), f32)

        @pl.when(s == 0)
        def _():
            for c in range(1, 3):
                fetch(c)

        @pl.when(s == chunks)
        def _():
            down_copy.start()
            acc[...] = jnp.zeros_like(acc)
            stat[...] = jnp.zeros_like(stat)

        @pl.when(s == plan.partials)
        def _():
            down_copy.wait()

    def hidden_slot(s):
        for order in (0, 1):
            d = (order + 1 - upper) % 2
            p = place(d)

            @pl.when((p == 0) & (s == plan.a))
            def _():
                def send(j, carry):
                    hidden_copy(d, j).start()
                    return carry

                lax.fori_loop(0, LEAD, send, 0)

            ahead = s + LEAD - plan.a

            @pl.when((p == 0) & (s >= plan.a) & (ahead < plan.early))
            def _():
                hidden_copy(d, ahead).start()

            ahead = s + LEAD - plan.b

            @pl.when((p == 0) & (ahead >= 0) & (ahead < plan.stripes - plan.early))
            def _():
                hidden_copy(d, ahead + plan.early).start()

        def stripe(t):
            k = jnp.where(t < plan.b, t - plan.a, t - plan.b + plan.early)
            return k, ((t >= plan.a) & (t < plan.a + plan.early)) | ((t >= plan.b) & (k < plan.stripes))

        for step in (hidden_pass, hidden_use):
            for order in (0, 1):
                d = (order + 1 - upper) % 2
                held = 2 if order and step is hidden_use else 0
                k, live = stripe(s - ROW_LAG * place(d) - held)

                @pl.when(live)
                def _():
                    step(d, k)

        every = BLOCK // STRIPE
        done = s - ROW_LAG * jnp.maximum(r, n - 1 - r)
        send_at, live = stripe(done)

        @pl.when(live & (lax.rem(send_at, every) == every - 1) & (send_at < plan.stripes - every))
        def _():
            send_branch(lax.div(send_at, every))

        sum_at, sums = stripe(done - plan.sum_after)

        @pl.when(sums & (lax.rem(sum_at, every) == every - 1) & (sum_at < plan.stripes - 2 * every))
        def _():
            sum_branch(lax.div(sum_at, every))

        for h in (0, 1):
            inner = (r > 0) & (r < n - 1)
            last = plan.stripes - 1 - jnp.where(inner, 0, (1 - h) * every // 2)

            @pl.when(live & (send_at == last))
            def _():
                send_half(h)

    def first_slots(s, carry):
        partial_slot(s)
        return carry

    def mixed_slots(s, carry):
        partial_slot(s)
        hidden_slot(s)
        return carry

    def last_slots(s, carry):
        hidden_slot(s)
        return carry

    lax.fori_loop(0, plan.a, first_slots, 0)
    lax.fori_loop(plan.a, plan.tail, mixed_slots, 0)
    lax.fori_loop(plan.tail, plan.slots, last_slots, 0)
    sum_branch(blocks - 1)
    sum_half(0)

    for d in (0, 1):
        @pl.when(place(d) < n - 1)
        def _():
            square_copy(d).wait_send()
            for buffer, sem in ((sbuf.at[d], psend.at[d]), (hid.at[1 - d], hsend.at[d])):
                pltpu.make_async_remote_copy(
                    src_ref=buffer, dst_ref=buffer, send_sem=sem, recv_sem=ring.at[d, 0],
                    device_id=onward(d), device_id_type=MESH,
                ).wait_send()

    for k in range(1, m):
        for buffer, sem in ((brecv.at[:, k], bss), (bout, oss)):
            pltpu.make_async_remote_copy(
                src_ref=buffer, dst_ref=buffer, send_sem=sem.at[k - 1], recv_sem=osr.at[k - 1],
                device_id=somewhere(0, k), device_id_type=MESH,
            ).wait_send()

    sum_half(1)

    share = branch_ref.at[pl.ds(0, rows // m)]
    for k in range(1, m):
        for buffer, sem in ((hrecv_rows.at[:, k], hss), (hout, hos)):
            pltpu.make_async_remote_copy(
                src_ref=buffer, dst_ref=buffer, send_sem=sem.at[k - 1], recv_sem=osr.at[k - 1],
                device_id=somewhere(0, k), device_id_type=MESH,
            ).wait_send()
        pltpu.make_async_remote_copy(
            src_ref=share, dst_ref=share, send_sem=oss.at[k - 1], recv_sem=osr.at[k - 1],
            device_id=somewhere(0, k), device_id_type=MESH,
        ).wait_recv()
    pltpu.make_async_copy(share, share, osl).wait()
    all_stats = stat_ref.at[pl.ds(0, len(others))]
    both = pltpu.make_async_remote_copy(
        src_ref=all_stats, dst_ref=all_stats, send_sem=sts, recv_sem=str_,
        device_id=somewhere(0, 1), device_id_type=MESH,
    )
    both.wait_send()
    both.wait_recv()
    keep_stat.wait()


def finish_kernel(
    n, m, tok_hbm, branch_hbm, stat_hbm, post_hbm, out_hbm,
    tok, branch, stat, post, scale, out, isem, osem,
):
    rows, width = tok.shape
    parts = rows // PART
    blocks = rows // BLOCK - 1
    own_rows = BLOCK // m
    half_own = own_rows // 2
    f32 = jnp.float32
    stat_copy = pltpu.make_async_copy(stat_hbm, stat, isem.at[2 * parts])
    post_copy = pltpu.make_async_copy(post_hbm, post, isem.at[2 * parts + 1])
    stat_copy.start()
    post_copy.start()
    copies = []
    for q in range(parts):
        at = pl.ds(q * PART, PART)
        pair = (
            pltpu.make_async_copy(branch_hbm.at[at], branch.at[at], isem.at[q]),
            pltpu.make_async_copy(tok_hbm.at[at], tok.at[at], isem.at[parts + q]),
        )
        for copy in pair:
            copy.start()
        copies.append(pair)
    stat_copy.wait()
    for k in range(m):
        total = stat[k]
        for i in range(1, n):
            total = total + stat[i * m + k]
        inv = lax.rsqrt(total / (width * n) + epsilon)
        column = jnp.broadcast_to(inv, (LANES, rows // m)).T
        for b in range(blocks):
            scale[pl.ds(b * BLOCK + k * own_rows, own_rows), :] = column[b * own_rows:(b + 1) * own_rows]
        for h in (0, 1):
            first = blocks * own_rows + h * half_own
            to = pl.ds(blocks * BLOCK + h * (BLOCK // 2) + k * half_own, half_own)
            scale[to, :] = column[first:first + half_own]
    post_copy.wait()
    writes = []
    for q in range(parts):
        for copy in copies[q]:
            copy.wait()
        at = pl.ds(q * PART, PART)
        by = scale[at, :]
        for t in range(width // LANES):
            lanes = pl.ds(t * LANES, LANES)
            mixed = residual_scale * tok[at, lanes].astype(f32) + branch[at, lanes].astype(f32) * by * post[:, lanes]
            out[at, lanes] = mixed.astype(out.dtype)
        write = pltpu.make_async_copy(out.at[at], out_hbm.at[at], osem.at[q])
        write.start()
        writes.append(write)
    for write in writes:
        write.wait()


def local(n, m, tokens, pre_gain, w_gate, w_up, conv_gate, conv_up, w_down, post_gain):
    rows, width = tokens.shape[1:]
    chunks = w_gate.shape[1] // (2 * LANES)
    plan = Plan(n, rows, chunks)
    parts, blocks = plan.parts, plan.blocks
    own_rows = BLOCK // m
    wire = jnp.bfloat16 if n <= 4 else jnp.float32
    f32, bf16 = jnp.float32, jnp.bfloat16
    hbm = pl.BlockSpec(memory_space=pl.ANY)
    dma = pltpu.SemaphoreType.DMA
    branch, stat = pl.pallas_call(
        functools.partial(kernel, n, m, plan),
        out_shape=[
            jax.ShapeDtypeStruct((rows, width), bf16),
            jax.ShapeDtypeStruct((n * m, 1, rows // m), f32),
        ],
        in_specs=[hbm] * 7,
        out_specs=[hbm] * 2,
        scratch_shapes=[
            pltpu.VMEM((rows, width), bf16),
            pltpu.VMEM((1, width), f32),
            pltpu.VMEM(conv_gate.shape, f32),
            pltpu.VMEM(conv_up.shape, f32),
            pltpu.VMEM((chunks, 2, width, 2 * LANES), bf16),
            pltpu.VMEM(w_down.shape, bf16),
            pltpu.VMEM((rows, width), bf16),
            pltpu.VMEM((2, chunks, rows, 2 * LANES), wire),
            pltpu.VMEM((2, chunks, rows, 2 * LANES), wire),
            pltpu.VMEM((chunks, rows + 16, 2 * LANES), f32),
            pltpu.VMEM((2, rows, chunks * LANES), bf16),
            pltpu.VMEM((rows, width), f32),
            pltpu.VMEM((8, rows), f32),
            pltpu.VMEM((2, 8, rows), f32),
            pltpu.VMEM((2, 8, rows), f32),
            pltpu.VMEM((rows + 16, LANES), f32),
            pltpu.VMEM((rows, width), wire),
            pltpu.VMEM((blocks, m, own_rows, width), wire),
            pltpu.VMEM((blocks, own_rows, width), bf16),
            pltpu.VMEM((2, m, own_rows // 2, width), wire),
            pltpu.VMEM((2, m, own_rows // 2, width), wire),
            pltpu.VMEM((2, own_rows // 2, width), bf16),
            pltpu.VMEM((1, rows // m), f32),
            dma((parts + 3,)), dma((4,)), dma,
            dma((2,)), dma((2, PART // FIRST)), dma((2, plan.ring)), dma((2,)),
            dma((2,)), dma((2,)), dma((m - 1,)), dma((blocks,)), dma((m - 1,)), dma((m - 1,)), dma,
            dma((m - 1,)), dma((2,)), dma((m - 1,)), dma, dma, dma,
        ],
        compiler_params=pltpu.CompilerParams(
            collective_id=0, has_side_effects=True, vmem_limit_bytes=60 * 1024 * 1024
        ),
    )(tokens[0], pre_gain[None], w_gate, w_up, conv_gate, conv_up, w_down)
    out = pl.pallas_call(
        functools.partial(finish_kernel, n, m),
        out_shape=jax.ShapeDtypeStruct((rows, width), bf16),
        in_specs=[hbm] * 4,
        out_specs=hbm,
        scratch_shapes=[
            pltpu.VMEM((rows, width), bf16),
            pltpu.VMEM((rows, width), bf16),
            pltpu.VMEM((n * m, 1, rows // m), f32),
            pltpu.VMEM((1, width), f32),
            pltpu.VMEM((rows, LANES), f32),
            pltpu.VMEM((rows, width), bf16),
            dma((2 * parts + 2,)), dma((parts,)),
        ],
    )(tokens[0], branch, stat, post_gain[None])
    return out[None]


def solution(mesh):
    in_specs = (
        P("dp", None, "ra"),
        P("ra"),
        P("ra", "cb"),
        P("ra", "cb"),
        P(None, "cb"),
        P(None, "cb"),
        P("cb", "ra"),
        P("ra"),
    )
    out_specs = P("dp", None, "ra")
    return jax.shard_map(
        functools.partial(local, mesh.shape["ra"], mesh.shape["cb"]),
        mesh=mesh, in_specs=in_specs, out_specs=out_specs, check_vma=False,
    )
```

```python
import functools
import jax
import jax.numpy as jnp
from jax import lax
from jax.experimental import pallas as pl
from jax.experimental.pallas import tpu as pltpu
from jax.sharding import PartitionSpec as P

epsilon = 1e-06
residual_scale = 0.125
LANES = 128
PART = 128
BLOCK = 64
STRIPE = 16
LAG = 3
ROW_LAG = 4
LEAD = 5
FIRST = 32
PIECE = 32
MESH = pl.DeviceIdType.MESH


def gelu(v):
    return 0.5 * v * (1.0 + jnp.tanh(0.7978845608028654 * (v + 0.044715 * v * v * v)))


class Plan:
    def __init__(self, n, rows, chunks):
        self.parts = rows // PART
        self.head = self.parts - 1
        self.blocks = rows // BLOCK - 1
        self.upper = chunks * self.head
        self.partials = chunks * self.parts
        self.cut = self.head * PART - PIECE
        self.stripes = rows // STRIPE
        self.early = self.cut // STRIPE
        reach = LAG * (n - 1)
        self.a = max(self.partials, self.upper - 1 + reach)
        self.b = max(self.a + self.early, self.partials - 1 + reach + LEAD)
        self.ring = ROW_LAG * (n - 1) + LEAD + 3
        self.sum_after = 5
        self.tail = max(self.a, self.partials + reach)
        self.slots = self.b + self.stripes - self.early + ROW_LAG * (n - 1)


def kernel(
    n, m, plan,
    tok_hbm, pre_hbm, wg_hbm, wu_hbm, cg_hbm, cu_hbm, wd_hbm, branch_ref, stat_ref,
    tok, pre, cg, cu,
    w, wd, xw, rbuf, sbuf, full, hid, acc, sq_own, sq_out, sq_in, scale, bsend, brecv, bout, hsend_rows, hrecv_rows, hout, stat,
    lsem, wsem, dsem, psend, pfirst, ring, hsend, sqs, sqr, bss, bsr, oss, osr, osl, hss, hsr, hos, sts, str_, stl,
):
    rows, width = tok.shape
    wire = sbuf.dtype
    chunks = w.shape[0]
    half = chunks * LANES
    parts, blocks = plan.parts, plan.blocks
    own_rows = BLOCK // m
    half_own = own_rows // 2
    dim_full = width * n
    r = lax.axis_index("ra")
    me = lax.axis_index("cb")
    f32, bf16 = jnp.float32, jnp.bfloat16
    upper = (2 * r) // n

    def place(d):
        return r * (1 - d) + (n - 1 - r) * d

    def onward(d):
        return {"ra": (r + 1 - 2 * d + n) % n}

    def somewhere(i, k):
        return {"ra": (r + i) % n, "cb": (me + k) % m}

    def weight_copies(d, c):
        at = pl.ds(pl.multiple_of(d * half + c * LANES, LANES), LANES)
        return (
            pltpu.make_async_copy(wg_hbm.at[:, at], w.at[c, d, :, pl.ds(0, LANES)], wsem.at[lax.rem(c, 4)]),
            pltpu.make_async_copy(wu_hbm.at[:, at], w.at[c, d, :, pl.ds(LANES, LANES)], wsem.at[lax.rem(c, 4)]),
        )

    tok_copies = [
        pltpu.make_async_copy(tok_hbm.at[pl.ds(q * PART, PART)], tok.at[pl.ds(q * PART, PART)], lsem.at[q])
        for q in range(parts)
    ]
    pre_copy = pltpu.make_async_copy(pre_hbm, pre, lsem.at[parts])
    rest = [
        pltpu.make_async_copy(cg_hbm, cg, lsem.at[parts + 1]),
        pltpu.make_async_copy(cu_hbm, cu, lsem.at[parts + 2]),
    ]
    pre_copy.start()
    tok_copies[0].start()
    for d in (0, 1):
        for copy in weight_copies(d, 0):
            copy.start()
    for copy in tok_copies[1:]:
        copy.start()

    barrier = pltpu.get_barrier_semaphore()
    others = [(i, k) for k in range(m) for i in range(n) if i or k]

    for d in (0, 1):
        @pl.when(place(d) < n - 1)
        def _():
            pl.semaphore_signal(barrier, inc=1, device_id=onward(d), device_id_type=MESH)

    for k in range(1, m):
        pl.semaphore_signal(barrier, inc=1, device_id=somewhere(0, k), device_id_type=MESH)

    down_copy = pltpu.make_async_copy(wd_hbm, wd, dsem)

    def fetch(c):
        for d in (0, 1):
            for copy in weight_copies(d, c):
                copy.start()

    def square_copy(d):
        return pltpu.make_async_remote_copy(
            src_ref=sq_out.at[d], dst_ref=sq_in.at[d],
            send_sem=sqs.at[d], recv_sem=sqr.at[d],
            device_id=onward(d), device_id_type=MESH,
        )

    def own_squares():
        values = tok[...].astype(f32)
        square = values * values
        high = square.astype(bf16)
        low = (square - high.astype(f32)).astype(bf16)
        ones = jnp.ones((8, width), bf16)
        nt = (((1,), (1,)), ((), ()))
        sq_own[...] = lax.dot_general(ones, high, nt, preferred_element_type=f32) + lax.dot_general(
            ones, low, nt, preferred_element_type=f32
        )

    def square_step(d):
        p = place(d)

        @pl.when(p == 0)
        def _():
            sq_out[d] = sq_own[...]

        @pl.when(p > 0)
        def _():
            square_copy(d).wait_recv()
            sq_out[d] = sq_own[...] + sq_in[d]

        @pl.when(p < n - 1)
        def _():
            square_copy(d).start()

        @pl.when(p == n - 1)
        def _():
            inv = lax.rsqrt(sq_out[d] / dim_full + epsilon)
            scale[pl.ds(8, rows), :] = jnp.concatenate([inv] * (LANES // 8), axis=0).T

    def part_rows(b):
        return pl.ds(pl.multiple_of(b * PART, PART), PART)

    def block_rows(b):
        return pl.ds(pl.multiple_of(b * BLOCK, BLOCK), BLOCK)

    def partial_copy(d, i, c, b):
        at = part_rows(b)
        return pltpu.make_async_remote_copy(
            src_ref=sbuf.at[d, c, at], dst_ref=rbuf.at[d, c, at],
            send_sem=psend.at[d], recv_sem=ring.at[d, lax.rem(i, plan.ring)],
            device_id=onward(d), device_id_type=MESH,
        )

    def first_copy(d, j):
        at = pl.ds(j * FIRST, FIRST)
        return pltpu.make_async_remote_copy(
            src_ref=sbuf.at[d, 0, at], dst_ref=rbuf.at[d, 0, at],
            send_sem=psend.at[d], recv_sem=pfirst.at[d, j],
            device_id=onward(d), device_id_type=MESH,
        )

    def hidden_copy(d, k):
        at = pl.ds(pl.multiple_of(k * STRIPE, STRIPE), STRIPE)
        return pltpu.make_async_remote_copy(
            src_ref=hid.at[1 - d, at], dst_ref=hid.at[1 - d, at],
            send_sem=hsend.at[d], recv_sem=ring.at[d, lax.rem(plan.partials + k, plan.ring)],
            device_id=onward(d), device_id_type=MESH,
        )

    def finish_rows(d, c, low, high):
        at = pl.ds(pl.multiple_of(d * half + c * LANES, LANES), LANES)
        to = pl.ds(pl.multiple_of(c * LANES, LANES), LANES)
        taps_g, taps_u = cg[:, at], cu[:, at]
        for j in range(low, high, PIECE):
            by = scale[pl.ds(j, PIECE + 16), :]
            window = full[c, pl.ds(j, PIECE + 16), :] * jnp.concatenate([by, by], axis=1)
            before = pltpu.roll(window, 1, 0)[8:8 + PIECE]
            here = window[8:8 + PIECE]
            after = pltpu.roll(window, PIECE + 15, 0)[8:8 + PIECE]
            conv = []
            for side, taps in ((0, taps_g), (1, taps_u)):
                lanes = slice(side * LANES, (side + 1) * LANES)
                conv.append(
                    taps[0:1] * before[:, lanes] + taps[1:2] * here[:, lanes] + taps[2:3] * after[:, lanes]
                )
            hid[d, pl.ds(j, PIECE), to] = (gelu(conv[0]) * conv[1]).astype(bf16)

    def partial_step(d, i):
        p = place(d)
        c = jnp.where(i < plan.upper, lax.div(i, plan.head), i - plan.upper)
        b = jnp.where(i < plan.upper, lax.rem(i, plan.head), plan.head)
        at = part_rows(b)
        own = jnp.dot(xw[at, :], w[c, d], preferred_element_type=f32)

        @pl.when((p < n - 1) & (i == 0))
        def _():
            for j in range(PART // FIRST):
                some = pl.ds(j * FIRST, FIRST)
                piece = own[j * FIRST:(j + 1) * FIRST]

                @pl.when(p == 0)
                def _():
                    sbuf[d, 0, some] = piece.astype(wire)

                @pl.when(p > 0)
                def _():
                    first_copy(d, j).wait_recv()
                    sbuf[d, 0, some] = (piece + rbuf[d, 0, some].astype(f32)).astype(wire)

                first_copy(d, j).start()

        @pl.when((p == 0) & (i > 0))
        def _():
            sbuf[d, c, at] = own.astype(wire)
            partial_copy(d, i, c, b).start()

        @pl.when((p > 0) & (p < n - 1) & (i > 0))
        def _():
            partial_copy(d, i, c, b).wait_recv()
            sbuf[d, c, at] = (own + rbuf[d, c, at].astype(f32)).astype(wire)
            partial_copy(d, i, c, b).start()

        @pl.when(p == n - 1)
        def _():
            @pl.when(i == 0)
            def _():
                for j in range(PART // FIRST):
                    first_copy(d, j).wait_recv()

            @pl.when(i > 0)
            def _():
                partial_copy(d, i, c, b).wait_recv()

            full[c, pl.ds(pl.multiple_of(b * PART + 8, 8), PART), :] = own + rbuf[d, c, at].astype(f32)

            @pl.when(b == plan.head - 1)
            def _():
                finish_rows(d, c, 0, plan.cut)

            @pl.when(b == plan.head)
            def _():
                finish_rows(d, c, plan.cut, rows)

    def hidden_pass(d, k):
        p = place(d)

        @pl.when(p > 0)
        def _():
            hidden_copy(d, k).wait_recv()

        @pl.when((p > 0) & (p < n - 1))
        def _():
            hidden_copy(d, k).start()

    def hidden_use(d, k):
        every = BLOCK // STRIPE

        def product(at):
            acc[at, :] += jnp.dot(
                hid[1 - d, at, :], wd[pl.ds(pl.multiple_of((1 - d) * half, LANES), half), :],
                preferred_element_type=f32,
            )

        @pl.when((lax.rem(k, every) == every - 1) & (k < plan.stripes - every))
        def _():
            product(block_rows(lax.div(k, every)))

        ends = place(d) == n - 1

        @pl.when((k == plan.stripes - 1) & jnp.logical_not(ends))
        def _():
            product(pl.ds(rows - BLOCK, BLOCK))

        for h in (0, 1):
            @pl.when((k == plan.stripes - 1 - (1 - h) * every // 2) & ends)
            def _():
                product(pl.ds(rows - BLOCK + h * BLOCK // 2, BLOCK // 2))

    def mine(b):
        return pl.ds(pl.multiple_of(b * BLOCK + me * own_rows, own_rows), own_rows)

    def branch_copy(b, k):
        peer = (me + k) % m
        at = pl.ds(pl.multiple_of(b * BLOCK + peer * own_rows, own_rows), own_rows)
        return pltpu.make_async_remote_copy(
            src_ref=bsend.at[at], dst_ref=brecv.at[b, k],
            send_sem=bss.at[k - 1], recv_sem=bsr.at[b],
            device_id={"cb": peer}, device_id_type=MESH,
        )

    def out_copy(b, k):
        return pltpu.make_async_remote_copy(
            src_ref=bout.at[b], dst_ref=branch_ref.at[mine(b)],
            send_sem=oss.at[k - 1], recv_sem=osr.at[k - 1],
            device_id={"cb": (me + k) % m}, device_id_type=MESH,
        )

    def stat_copy(i, k):
        return pltpu.make_async_remote_copy(
            src_ref=stat, dst_ref=stat_ref.at[r * m + me],
            send_sem=sts, recv_sem=str_,
            device_id=somewhere(i, k), device_id_type=MESH,
        )

    keep_stat = pltpu.make_async_copy(stat, stat_ref.at[r * m + me], stl)

    def send_branch(b):
        at = block_rows(b)
        bsend[at, :] = acc[at, :].astype(wire)
        for k in range(1, m):
            branch_copy(b, k).start()

    def half_row(h, peer):
        return pl.ds(pl.multiple_of(rows - BLOCK + h * (BLOCK // 2) + peer * half_own, half_own), half_own)

    def half_copy(h, k):
        return pltpu.make_async_remote_copy(
            src_ref=hsend_rows.at[h, (me + k) % m], dst_ref=hrecv_rows.at[h, k],
            send_sem=hss.at[k - 1], recv_sem=hsr.at[h],
            device_id={"cb": (me + k) % m}, device_id_type=MESH,
        )

    def half_out(h, k):
        return pltpu.make_async_remote_copy(
            src_ref=hout.at[h], dst_ref=branch_ref.at[half_row(h, me)],
            send_sem=hos.at[k - 1], recv_sem=osr.at[k - 1],
            device_id={"cb": (me + k) % m}, device_id_type=MESH,
        )

    def keep_half(h):
        return pltpu.make_async_copy(hout.at[h], branch_ref.at[half_row(h, me)], osl)

    def send_half(h):
        for peer in range(m):
            hsend_rows[h, peer] = acc[half_row(h, peer), :].astype(wire)
        for k in range(1, m):
            half_copy(h, k).start()

    def add_stat(branch, first):
        sums = jnp.sum(branch * branch, axis=1, keepdims=True)
        shape = (branch.shape[0], stat.shape[1])
        lane = lax.broadcasted_iota(jnp.int32, shape, 1)
        row = lax.broadcasted_iota(jnp.int32, shape, 0)
        spread = jnp.sum(jnp.where(lane == first + row, sums, 0.0), axis=0, keepdims=True)
        stat[...] = stat[...] + spread

    def sum_half(h):
        incoming = hrecv_rows.at[h, pl.ds(1, m - 1)]
        pltpu.make_async_copy(incoming, incoming, hsr.at[h]).wait()
        branch = acc[half_row(h, me), :]
        for k in range(1, m):
            branch = branch + hrecv_rows[h, k].astype(f32)
        add_stat(branch, rows // m - own_rows + h * half_own)
        if h:
            for k in (2, 1, 3, 0) if m == 4 else range(m):
                for j in range(n):
                    i = (n - 1 - 2 * r + j + 2 * n) % n

                    @pl.when((i != 0) | (k != 0))
                    def _():
                        stat_copy(i, k).start()
            keep_stat.start()
        hout[h] = branch.astype(bf16)
        for k in range(1, m):
            half_out(h, k).start()
        keep_half(h).start()

    def sum_branch(b):
        branch = acc[mine(b), :]
        incoming = brecv.at[b, pl.ds(1, m - 1)]
        pltpu.make_async_copy(incoming, incoming, bsr.at[b]).wait()
        for k in range(1, m):
            branch = branch + brecv[b, k].astype(f32)
        bout[b] = branch.astype(bf16)
        for k in range(1, m):
            out_copy(b, k).start()
        pltpu.make_async_copy(bout.at[b], branch_ref.at[mine(b)], osl).start()
        add_stat(branch, b * own_rows)

    pre_copy.wait()

    def partial_slot(s):
        def take(q):
            at = part_rows(q)
            pltpu.make_async_copy(tok_hbm.at[at], tok.at[at], lsem.at[q]).wait()
            xw[at, :] = (tok[at, :].astype(f32) * pre[...]).astype(bf16)

        @pl.when(s < plan.head)
        def _():
            take(jnp.minimum(s, parts - 1))

        @pl.when(s == 0)
        def _():
            pl.semaphore_wait(barrier, jnp.where((r == 0) | (r == n - 1), 1, 2) + m - 1)

        @pl.when(s == plan.head - 1)
        def _():
            take(plan.head)
            for copy in rest:
                copy.wait()
            own_squares()

        t = s - LAG * jnp.minimum(r, n - 1 - r)

        @pl.when((t >= 0) & (t < plan.upper) & (lax.rem(t, plan.head) == 0))
        def _():
            c = lax.div(t, plan.head)
            pltpu.make_async_copy(w.at[c], w.at[c], wsem.at[lax.rem(c, 4)]).wait()

            @pl.when(c + 3 < chunks)
            def _():
                fetch(c + 3)

        for order in (0, 1):
            d = (order + 1 - upper) % 2
            i = s - LAG * place(d)

            @pl.when(i == plan.head - 1)
            def _():
                square_step(d)

            @pl.when((i >= 0) & (i < plan.partials))
            def _():
                partial_step(d, i)

        @pl.when(s == 0)
        def _():
            for copy in rest:
                copy.start()
            for at in (0, rows + 8):
                scale[pl.ds(at, 8), :] = jnp.zeros((8, LANES), f32)
                for c in range(chunks):
                    full[c, pl.ds(at, 8), :] = jnp.zeros((8, 2 * LANES), f32)

        @pl.when(s == 0)
        def _():
            for c in range(1, 3):
                fetch(c)

        @pl.when(s == chunks)
        def _():
            down_copy.start()
            acc[...] = jnp.zeros_like(acc)
            stat[...] = jnp.zeros_like(stat)

        @pl.when(s == plan.partials)
        def _():
            down_copy.wait()

    def hidden_slot(s):
        for order in (0, 1):
            d = (order + 1 - upper) % 2
            p = place(d)

            @pl.when((p == 0) & (s == plan.a))
            def _():
                def send(j, carry):
                    hidden_copy(d, j).start()
                    return carry

                lax.fori_loop(0, LEAD, send, 0)

            ahead = s + LEAD - plan.a

            @pl.when((p == 0) & (s >= plan.a) & (ahead < plan.early))
            def _():
                hidden_copy(d, ahead).start()

            ahead = s + LEAD - plan.b

            @pl.when((p == 0) & (ahead >= 0) & (ahead < plan.stripes - plan.early))
            def _():
                hidden_copy(d, ahead + plan.early).start()

        def stripe(t):
            k = jnp.where(t < plan.b, t - plan.a, t - plan.b + plan.early)
            return k, ((t >= plan.a) & (t < plan.a + plan.early)) | ((t >= plan.b) & (k < plan.stripes))

        for step in (hidden_pass, hidden_use):
            for order in (0, 1):
                d = (order + 1 - upper) % 2
                held = 2 if order and step is hidden_use else 0
                k, live = stripe(s - ROW_LAG * place(d) - held)

                @pl.when(live)
                def _():
                    step(d, k)

        every = BLOCK // STRIPE
        done = s - ROW_LAG * jnp.maximum(r, n - 1 - r)
        send_at, live = stripe(done)

        @pl.when(live & (lax.rem(send_at, every) == every - 1) & (send_at < plan.stripes - every))
        def _():
            send_branch(lax.div(send_at, every))

        sum_at, sums = stripe(done - plan.sum_after)

        @pl.when(sums & (lax.rem(sum_at, every) == every - 1) & (sum_at < plan.stripes - 2 * every))
        def _():
            sum_branch(lax.div(sum_at, every))

        for h in (0, 1):
            inner = (r > 0) & (r < n - 1)
            last = plan.stripes - 1 - jnp.where(inner, 0, (1 - h) * every // 2)

            @pl.when(live & (send_at == last))
            def _():
                send_half(h)

    def first_slots(s, carry):
        partial_slot(s)
        return carry

    def mixed_slots(s, carry):
        partial_slot(s)
        hidden_slot(s)
        return carry

    def last_slots(s, carry):
        hidden_slot(s)
        return carry

    lax.fori_loop(0, plan.a, first_slots, 0)
    lax.fori_loop(plan.a, plan.tail, mixed_slots, 0)
    lax.fori_loop(plan.tail, plan.slots, last_slots, 0)
    sum_branch(blocks - 1)
    sum_half(0)

    for d in (0, 1):
        @pl.when(place(d) < n - 1)
        def _():
            square_copy(d).wait_send()
            for buffer, sem in ((sbuf.at[d], psend.at[d]), (hid.at[1 - d], hsend.at[d])):
                pltpu.make_async_remote_copy(
                    src_ref=buffer, dst_ref=buffer, send_sem=sem, recv_sem=ring.at[d, 0],
                    device_id=onward(d), device_id_type=MESH,
                ).wait_send()

    for k in range(1, m):
        for buffer, sem in ((brecv.at[:, k], bss), (bout, oss)):
            pltpu.make_async_remote_copy(
                src_ref=buffer, dst_ref=buffer, send_sem=sem.at[k - 1], recv_sem=osr.at[k - 1],
                device_id=somewhere(0, k), device_id_type=MESH,
            ).wait_send()

    sum_half(1)

    share = branch_ref.at[pl.ds(0, rows // m)]
    for k in range(1, m):
        for buffer, sem in ((hrecv_rows.at[:, k], hss), (hout, hos)):
            pltpu.make_async_remote_copy(
                src_ref=buffer, dst_ref=buffer, send_sem=sem.at[k - 1], recv_sem=osr.at[k - 1],
                device_id=somewhere(0, k), device_id_type=MESH,
            ).wait_send()
        pltpu.make_async_remote_copy(
            src_ref=share, dst_ref=share, send_sem=oss.at[k - 1], recv_sem=osr.at[k - 1],
            device_id=somewhere(0, k), device_id_type=MESH,
        ).wait_recv()
    pltpu.make_async_copy(share, share, osl).wait()
    all_stats = stat_ref.at[pl.ds(0, len(others))]
    both = pltpu.make_async_remote_copy(
        src_ref=all_stats, dst_ref=all_stats, send_sem=sts, recv_sem=str_,
        device_id=somewhere(0, 1), device_id_type=MESH,
    )
    both.wait_send()
    both.wait_recv()
    keep_stat.wait()


def finish_kernel(
    n, m, tok_hbm, branch_hbm, stat_hbm, post_hbm, out_hbm,
    tok, branch, stat, post, scale, out, isem, osem,
):
    rows, width = tok.shape
    parts = rows // PART
    blocks = rows // BLOCK - 1
    own_rows = BLOCK // m
    half_own = own_rows // 2
    f32 = jnp.float32
    stat_copy = pltpu.make_async_copy(stat_hbm, stat, isem.at[2 * parts])
    post_copy = pltpu.make_async_copy(post_hbm, post, isem.at[2 * parts + 1])
    stat_copy.start()
    post_copy.start()
    copies = []
    for q in range(parts):
        at = pl.ds(q * PART, PART)
        pair = (
            pltpu.make_async_copy(branch_hbm.at[at], branch.at[at], isem.at[q]),
            pltpu.make_async_copy(tok_hbm.at[at], tok.at[at], isem.at[parts + q]),
        )
        for copy in pair:
            copy.start()
        copies.append(pair)
    stat_copy.wait()
    for k in range(m):
        total = stat[k]
        for i in range(1, n):
            total = total + stat[i * m + k]
        inv = lax.rsqrt(total / (width * n) + epsilon)
        column = jnp.broadcast_to(inv, (LANES, rows // m)).T
        for b in range(blocks):
            scale[pl.ds(b * BLOCK + k * own_rows, own_rows), :] = column[b * own_rows:(b + 1) * own_rows]
        for h in (0, 1):
            first = blocks * own_rows + h * half_own
            to = pl.ds(blocks * BLOCK + h * (BLOCK // 2) + k * half_own, half_own)
            scale[to, :] = column[first:first + half_own]
    post_copy.wait()
    writes = []
    for q in range(parts):
        for copy in copies[q]:
            copy.wait()
        at = pl.ds(q * PART, PART)
        by = scale[at, :]
        for t in range(width // LANES):
            lanes = pl.ds(t * LANES, LANES)
            mixed = residual_scale * tok[at, lanes].astype(f32) + branch[at, lanes].astype(f32) * by * post[:, lanes]
            out[at, lanes] = mixed.astype(out.dtype)
        write = pltpu.make_async_copy(out.at[at], out_hbm.at[at], osem.at[q])
        write.start()
        writes.append(write)
    for write in writes:
        write.wait()


def local(n, m, tokens, pre_gain, w_gate, w_up, conv_gate, conv_up, w_down, post_gain):
    rows, width = tokens.shape[1:]
    chunks = w_gate.shape[1] // (2 * LANES)
    plan = Plan(n, rows, chunks)
    parts, blocks = plan.parts, plan.blocks
    own_rows = BLOCK // m
    wire = jnp.bfloat16 if n <= 4 else jnp.float32
    f32, bf16 = jnp.float32, jnp.bfloat16
    hbm = pl.BlockSpec(memory_space=pl.ANY)
    dma = pltpu.SemaphoreType.DMA
    branch, stat = pl.pallas_call(
        functools.partial(kernel, n, m, plan),
        out_shape=[
            jax.ShapeDtypeStruct((rows, width), bf16),
            jax.ShapeDtypeStruct((n * m, 1, rows // m), f32),
        ],
        in_specs=[hbm] * 7,
        out_specs=[hbm] * 2,
        scratch_shapes=[
            pltpu.VMEM((rows, width), bf16),
            pltpu.VMEM((1, width), f32),
            pltpu.VMEM(conv_gate.shape, f32),
            pltpu.VMEM(conv_up.shape, f32),
            pltpu.VMEM((chunks, 2, width, 2 * LANES), bf16),
            pltpu.VMEM(w_down.shape, bf16),
            pltpu.VMEM((rows, width), bf16),
            pltpu.VMEM((2, chunks, rows, 2 * LANES), wire),
            pltpu.VMEM((2, chunks, rows, 2 * LANES), wire),
            pltpu.VMEM((chunks, rows + 16, 2 * LANES), f32),
            pltpu.VMEM((2, rows, chunks * LANES), bf16),
            pltpu.VMEM((rows, width), f32),
            pltpu.VMEM((8, rows), f32),
            pltpu.VMEM((2, 8, rows), f32),
            pltpu.VMEM((2, 8, rows), f32),
            pltpu.VMEM((rows + 16, LANES), f32),
            pltpu.VMEM((rows, width), wire),
            pltpu.VMEM((blocks, m, own_rows, width), wire),
            pltpu.VMEM((blocks, own_rows, width), bf16),
            pltpu.VMEM((2, m, own_rows // 2, width), wire),
            pltpu.VMEM((2, m, own_rows // 2, width), wire),
            pltpu.VMEM((2, own_rows // 2, width), bf16),
            pltpu.VMEM((1, rows // m), f32),
            dma((parts + 3,)), dma((4,)), dma,
            dma((2,)), dma((2, PART // FIRST)), dma((2, plan.ring)), dma((2,)),
            dma((2,)), dma((2,)), dma((m - 1,)), dma((blocks,)), dma((m - 1,)), dma((m - 1,)), dma,
            dma((m - 1,)), dma((2,)), dma((m - 1,)), dma, dma, dma,
        ],
        compiler_params=pltpu.CompilerParams(
            collective_id=0, has_side_effects=True, vmem_limit_bytes=60 * 1024 * 1024
        ),
    )(tokens[0], pre_gain[None], w_gate, w_up, conv_gate, conv_up, w_down)
    out = pl.pallas_call(
        functools.partial(finish_kernel, n, m),
        out_shape=jax.ShapeDtypeStruct((rows, width), bf16),
        in_specs=[hbm] * 4,
        out_specs=hbm,
        scratch_shapes=[
            pltpu.VMEM((rows, width), bf16),
            pltpu.VMEM((rows, width), bf16),
            pltpu.VMEM((n * m, 1, rows // m), f32),
            pltpu.VMEM((1, width), f32),
            pltpu.VMEM((rows, LANES), f32),
            pltpu.VMEM((rows, width), bf16),
            dma((2 * parts + 2,)), dma((parts,)),
        ],
    )(tokens[0], branch, stat, post_gain[None])
    return out[None]


def solution(mesh):
    in_specs = (
        P("dp", None, "ra"),
        P("ra"),
        P("ra", "cb"),
        P("ra", "cb"),
        P(None, "cb"),
        P(None, "cb"),
        P("cb", "ra"),
        P("ra"),
    )
    out_specs = P("dp", None, "ra")
    return jax.shard_map(
        functools.partial(local, mesh.shape["ra"], mesh.shape["cb"]),
        mesh=mesh, in_specs=in_specs, out_specs=out_specs, check_vma=False,
    )
```
